32 devices in a mesh: fs: 8 (over z, x), tp: 4 (over y, core).
Axes of the slice: x: 2, y: 2, z: 4, core: 2. Of those that a mesh axis runs over, the one named last changes fastest.
Arguments:
- tokens: bfloat16 [8192, 2048], P('fs', 'tp'), may hold values from -17 to 17
- first_gain: float32 [2048], replicated, may hold values from 0.1 to 1.9
- first_gate: bfloat16 [2048, 5120], P('fs', 'tp'), may hold values from -0.125 to 0.125
- first_up: bfloat16 [2048, 5120], P('fs', 'tp'), may hold values from -0.125 to 0.125
- first_down: bfloat16 [2048, 5120], P('fs', 'tp'), may hold values from -0.078125 to 0.078125
- mix_gain: float32 [2048], replicated, may hold values from 0.1 to 1.9
- mix_input: bfloat16 [2048, 1024], P('fs', 'tp'), may hold values from -0.125 to 0.125
- mix_branch: bfloat16 [2048, 1024], P('fs', 'tp'), may hold values from -0.125 to 0.125
- conv_weight: bfloat16 [4, 1024], P(None, 'tp'), may hold values from -3 to 3
- rate_weight: bfloat16 [16, 64, 64], P('tp'), may hold values from -0.75 to 0.75
- input_weight: bfloat16 [16, 64, 64], P('tp'), may hold values from -0.75 to 0.75
- decay_param: float32 [1024], P('tp'), may hold values from 3 to 11
- decay_shift: float32 [8192, 16], P('fs', 'tp'), may hold values from -1.5 to 0
- mix_output: bfloat16 [2048, 1024], P('fs', 'tp'), may hold values from -0.1875 to 0.1875
- second_gain: float32 [2048], replicated, may hold values from 0.1 to 1.9
- second_gate: bfloat16 [2048, 5120], P('fs', 'tp'), may hold values from -0.125 to 0.125
- second_up: bfloat16 [2048, 5120], P('fs', 'tp'), may hold values from -0.125 to 0.125
- second_down: bfloat16 [2048, 5120], P('fs', 'tp'), may hold values from -0.078125 to 0.078125
- final_gain: float32 [2048], P('tp'), may hold values from 0.1 to 1.9
Outputs:
- output: bfloat16 [8192, 2048], P('fs', 'tp')
The draws below stay inside these ranges and needn't reach their ends.
All inputs are finite; a program needn't handle non-finite values.
Results may differ from the reference program's by a relative error of at most 0.019.
Values may be sent and summed in bfloat16 or wider, within the bound.
A program may use at most 128 MiB of HBM per device.

```python
import math
import jax
import jax.numpy as jnp
from jax import lax

D = 2048
FF = 5120
LANE_GROUPINGS = 16
HEAD_DIM = 64
CONV = 4
SEQ = 1024
LRU = 1024
SYMBOL_TOTAL = 8192
N_TP = 4


def draw_tokens(key, part):
    key_base, key_rows = jax.random.split(key, 2)
    starting_number = jnp.clip(jax.random.normal(key_base, (SYMBOL_TOTAL, D), jnp.float32), -4.0, 4.0)
    rows = jnp.exp(jax.random.uniform(key_rows, (SYMBOL_TOTAL, 1), jnp.float32, 0.0, math.log(4.0)))
    columns = jnp.exp(math.log(3.0) * jnp.arange(D, dtype=jnp.float32) / D)
    return (0.25 * starting_number * rows * columns[None, :]).astype(jnp.bfloat16)


def draw_decay_param(key, part):
    key_pick, key_rate = jax.random.split(key, 2)
    share = 0.5
    picked = jax.random.uniform(key_pick, (LRU,), jnp.float32) < share
    unit = jax.random.uniform(key_rate, (LRU,), jnp.float32)
    slow = jnp.exp(math.log(0.5) + unit * math.log(4.0)) / (4.0 * SEQ)
    fast = jnp.exp(math.log(1.0 / 120.0) + unit * math.log(5.0))
    speed = jnp.where(picked, slow, fast)
    return -speed - jnp.log(-jnp.expm1(-speed))


def draw_decay_shift(key, part):
    key_base, key_spot, key_depth = jax.random.split(key, 3)
    count = SYMBOL_TOTAL // SEQ
    starting_number = -jnp.exp(jax.random.uniform(key_base, (count, 1, LANE_GROUPINGS), jnp.float32, math.log(0.1), math.log(0.5))) / SEQ
    location_marks = jax.random.randint(key_spot, (count, 2, 1), 0, SEQ)
    layer_ordinal = jnp.log(jax.random.uniform(key_depth, (count, 2, 1), jnp.float32, 0.5, 0.8))
    position_holders = jnp.arange(SEQ, dtype=jnp.int32)[None, None, :]
    repeated_spans = jnp.sum(jnp.where(location_marks == position_holders, layer_ordinal, 0.0), axis=1)
    return (starting_number + repeated_spans[:, :, None]).reshape(SYMBOL_TOTAL, LANE_GROUPINGS)


def steps_of(own_key, extent, pieces, low, largest):
    loudness, own = 1.0, jax.random.fold_in(own_key, 6)
    for axis_at, parts in pieces:
        steps = jnp.exp(jax.random.uniform(jax.random.fold_in(own, axis_at), (parts,), jnp.float32, low / len(pieces), largest / len(pieces)))
        loudness = loudness * jnp.repeat(steps, extent[axis_at] // parts).reshape([-1 if axis == axis_at else 1 for axis in range(len(extent))])
    return loudness


def noise(own_key, shape, spread, bound, cuts=(), kind=jnp.bfloat16):
    entries = jax.random.normal(own_key, shape, jnp.float32) * spread
    if len(cuts) > 0:
        entries = steps_of(own_key, shape, cuts, -0.22, 0.18) * entries
    return jnp.clip(entries, min=-bound, max=bound).astype(kind)


def setup_inputs(seed: int = 0) -> dict:
    streams_of = jax.random.split(jax.random.key(seed), 20)
    tokens = draw_tokens(jax.random.fold_in(streams_of[19], 71), 0)
    first_gain = jnp.clip(1.0 + 0.18 * jax.random.normal(streams_of[1], (D,), jnp.float32), 0.1, 1.9)
    first_gate = noise(streams_of[2], (D, FF), D ** -0.5, 0.125, ((0, 8), (1, 4)))
    first_up = noise(streams_of[3], (D, FF), D ** -0.5, 0.125, ((0, 8), (1, 4)))
    first_down = noise(streams_of[4], (D, FF), FF ** -0.5, 0.078125, ((0, 8), (1, 4)))
    mix_gain = jnp.clip(1.0 + 0.18 * jax.random.normal(streams_of[5], (D,), jnp.float32), 0.1, 1.9)
    mix_input = noise(streams_of[6], (D, LRU), D ** -0.5, 0.125, ((0, 8), (1, 4)))
    mix_branch = noise(streams_of[7], (D, LRU), D ** -0.5, 0.125, ((0, 8), (1, 4)))
    conv_weight = noise(streams_of[8], (CONV, LRU), CONV ** -0.5, 3.0, ((1, 4),))
    rate_weight = noise(streams_of[9], (LANE_GROUPINGS, HEAD_DIM, HEAD_DIM), HEAD_DIM ** -0.5, 0.75, ((0, 4),))
    input_weight = noise(streams_of[10], (LANE_GROUPINGS, HEAD_DIM, HEAD_DIM), HEAD_DIM ** -0.5, 0.75, ((0, 4),))
    decay_param = draw_decay_param(jax.random.fold_in(streams_of[19], 71), 0)
    decay_shift = draw_decay_shift(jax.random.fold_in(streams_of[19], 71), 0)
    mix_output = noise(streams_of[13], (D, LRU), LRU ** -0.5, 0.1875, ((0, 8), (1, 4)))
    second_gain = jnp.clip(1.0 + 0.18 * jax.random.normal(streams_of[14], (D,), jnp.float32), 0.1, 1.9)
    second_gate = noise(streams_of[15], (D, FF), D ** -0.5, 0.125, ((0, 8), (1, 4)))
    second_up = noise(streams_of[16], (D, FF), D ** -0.5, 0.125, ((0, 8), (1, 4)))
    second_down = noise(streams_of[17], (D, FF), FF ** -0.5, 0.078125, ((0, 8), (1, 4)))
    final_gain = jnp.clip(1.0 + 0.18 * jax.random.normal(streams_of[18], (D,), jnp.float32), 0.1, 1.9)
    return dict(tokens=tokens, first_gain=first_gain, first_gate=first_gate, first_up=first_up, first_down=first_down, mix_gain=mix_gain, mix_input=mix_input, mix_branch=mix_branch, conv_weight=conv_weight, rate_weight=rate_weight, input_weight=input_weight, decay_param=decay_param, decay_shift=decay_shift, mix_output=mix_output, second_gain=second_gain, second_gate=second_gate, second_up=second_up, second_down=second_down, final_gain=final_gain)


norm_eps = 1e-06
rate_scale = 8.0

def rms_rows(rows, gain):
    values = rows.astype(jnp.float32)
    scale = lax.rsqrt(lax.optimization_barrier(jnp.mean(values * values, axis=-1, keepdims=True)) + norm_eps)
    return (values * scale * gain).astype(jnp.bfloat16)

def group_terms(left, weight):
    width = left.shape[1] // N_TP
    total = jnp.zeros((left.shape[0], weight.shape[0]), jnp.float32)
    for group in range(N_TP):
        piece = left[:, group * width:(group + 1) * width]
        weight_piece = weight[:, group * width:(group + 1) * width]
        term = lax.dot_general(piece, weight_piece, (((1,), (1,)), ((), ())), preferred_element_type=jnp.float32)
        total = total + lax.optimization_barrier(term.astype(jnp.bfloat16)).astype(jnp.float32)
    return total

def half_step(stream, gain, weight_gate, weight_up, weight_down):
    normed = rms_rows(stream, gain)
    gate_value = jnp.dot(normed, weight_gate, preferred_element_type=jnp.float32)
    up_value = jnp.dot(normed, weight_up, preferred_element_type=jnp.float32)
    hidden = (jax.nn.silu(gate_value) * up_value).astype(jnp.bfloat16)
    return (stream.astype(jnp.float32) + 0.5 * group_terms(hidden, weight_down)).astype(jnp.bfloat16)

def combine_steps(earlier, later):
    return (earlier[0] * later[0], later[0] * earlier[1] + later[1])

def lane_mixer(stream, gain, mix_input, mix_branch, conv_weight, rate_weight, input_weight, decay_param, decay_shift, mix_output):
    normed = rms_rows(stream, gain)
    lane_input = jnp.dot(normed, mix_input, preferred_element_type=jnp.float32).astype(jnp.bfloat16)
    branch_value = jnp.dot(normed, mix_branch, preferred_element_type=jnp.float32)
    width = lane_input.shape[1]
    lanes = lane_input.reshape(-1, SEQ, width).astype(jnp.float32)
    count = lanes.shape[0]
    padded = jnp.pad(lanes, ((0, 0), (CONV - 1, 0), (0, 0)))
    conv_sum = jnp.zeros_like(lanes)
    for offset in range(CONV):
        conv_sum = conv_sum + padded[:, offset:offset + SEQ] * conv_weight[offset].astype(jnp.float32)
    conv_out = conv_sum.astype(jnp.bfloat16)
    blocks = conv_out.reshape(count, SEQ, -1, HEAD_DIM).astype(jnp.float32)
    rate = jax.nn.sigmoid(jnp.einsum('nshd,hde->nshe', blocks, rate_weight.astype(jnp.float32))).reshape(lanes.shape)
    admit = jax.nn.sigmoid(jnp.einsum('nshd,hde->nshe', blocks, input_weight.astype(jnp.float32))).reshape(lanes.shape)
    shift = jnp.repeat(decay_shift.reshape(count, SEQ, -1), HEAD_DIM, axis=-1)
    log_decay = rate_scale * rate * jax.nn.log_sigmoid(decay_param) + shift
    drive = jnp.sqrt(-jnp.expm1(2.0 * log_decay)) * admit * conv_out.astype(jnp.float32)
    _, state = lax.associative_scan(combine_steps, (jnp.exp(log_decay), drive), axis=1)
    mixed_lane = (state.reshape(-1, width) * jax.nn.gelu(branch_value)).astype(jnp.bfloat16)
    return (stream.astype(jnp.float32) + group_terms(mixed_lane, mix_output)).astype(jnp.bfloat16)

def reference(tokens, first_gain, first_gate, first_up, first_down, mix_gain, mix_input, mix_branch, conv_weight, rate_weight, input_weight, decay_param, decay_shift, mix_output, second_gain, second_gate, second_up, second_down, final_gain):
    stream = half_step(tokens, first_gain, first_gate, first_up, first_down)
    stream = lane_mixer(stream, mix_gain, mix_input, mix_branch, conv_weight, rate_weight, input_weight, decay_param, decay_shift, mix_output)
    stream = half_step(stream, second_gain, second_gate, second_up, second_down)
    values = stream.astype(jnp.float32)
    scale = lax.rsqrt(lax.optimization_barrier(jnp.mean(values * values, axis=-1, keepdims=True)) + norm_eps)
    return (values * scale * final_gain).astype(jnp.bfloat16)
```

```python
import functools

import jax
import jax.numpy as jnp
from jax import lax
from jax.experimental import pallas as pl
from jax.experimental.pallas import tpu as pltpu
from jax.sharding import PartitionSpec as P

HEAD_DIM = 64
CONV = 4
norm_eps = 1e-06
rate_scale = 8.0
MESH = pl.DeviceIdType.MESH
F32, BF16 = jnp.float32, jnp.bfloat16
G1, U1, D1, MI, MB, MO, G2, U2, D2A, D2B = range(10)


def tile_of(size, *choices):
    for choice in choices:
        if size % choice == 0:
            return choice
    return size


def negative_expm1(y):
    series = 1.0 + y * (1.0 / 6.0)
    for k in (5, 4, 3, 2):
        series = 1.0 + y * (1.0 / k) * series
    return jnp.where(y > -0.25, -y * series, 1.0 - jnp.exp(y))


def dot(left, right):
    return jnp.dot(left, right, preferred_element_type=F32)


def dot_last(left, right):
    return lax.dot_general(left, right, (((1,), (1,)), ((), ())), preferred_element_type=F32)


def kernel(
    n,
    m,
    tokens,
    first_gate,
    first_up,
    first_down,
    mix_input,
    mix_branch,
    mix_output,
    second_gate,
    second_up,
    second_down,
    first_gain,
    mix_gain,
    second_gain,
    conv_weight,
    rate_weight,
    input_weight,
    decay_param,
    decay_shift,
    stream,
    scale_out,
    w_gate1,
    w_up1,
    w_down1,
    w_in,
    w_branch,
    w_out,
    w_gate2,
    w_up2,
    w_down2,
    gathered,
    normed,
    hidden,
    terms,
    near,
    far,
    mixed,
    lane,
    branch,
    decay,
    drive,
    rate_map,
    input_map,
    square_own,
    square_in,
    ring_send,
    ring_recv,
    own_sem,
    ag_near_send,
    ag_near_recv,
    ag_far_send,
    ag_far_recv,
    rs_near_send,
    rs_near_recv,
    rs_far_send,
    rs_far_recv,
    sq_send,
    sq_recv,
):
    h = n // 2
    chips = m // 2
    q = n // m
    rows, width = stream.shape
    d = width * m
    block = d // n
    units = first_gate.shape[1]
    lanes = mix_input.shape[1]
    fs = lax.axis_index("fs")
    tp = lax.axis_index("tp")
    chip = tp // 2
    core = tp % 2
    partner = tp + 1 - 2 * core
    at = jnp.where(fs % 2 == 0, fs // 2, n - 1 - fs // 2)

    def owner(place):
        p = lax.rem(place + 2 * n, n)
        return jnp.where(p < h, 2 * p, 2 * (n - 1 - p) + 1)

    right, left = owner(at + 1), owner(at - 1)
    half = block // 2
    plan = [
        (first_gate, w_gate1, 0, block),
        (first_up, w_up1, 0, block),
        (first_down, w_down1, 0, block),
        (mix_input, w_in, 0, block),
        (mix_branch, w_branch, 0, block),
        (mix_output, w_out, 0, block),
        (second_gate, w_gate2, 0, block),
        (second_up, w_up2, 0, block),
        (second_down, w_down2, 0, half),
        (second_down, w_down2, half, half),
    ]

    def ring_copy(k, way, step, arriving=False):
        source, buffer, low, count = plan[k]
        sign = -1 if way == 0 else 1
        b = owner(at + sign * (step + 1 if arriving else step))
        if step == h - 1:
            count = count // 2
            low = low + way * count
        place = pl.ds(pl.multiple_of(b * block + low, 16), count)
        if step == 0 and not arriving:
            src = source if count == block else source.at[pl.ds(low, count)]
        else:
            src = buffer.at[place]
        return pltpu.make_async_remote_copy(
            src_ref=src,
            dst_ref=buffer.at[place],
            send_sem=ring_send.at[k, way, step],
            recv_sem=ring_recv.at[k, way, step],
            device_id={"fs": right if way == 0 else left},
            device_id_type=MESH,
        )

    def launch(*ks):
        for k in ks:
            for way in (0, 1):
                ring_copy(k, way, 0).start()

    def serve(k, step):
        for way in (0, 1):
            ring_copy(k, way, step - 1, arriving=True).wait_recv()
            if step < h:
                ring_copy(k, way, step).start()

    barrier = pltpu.get_barrier_semaphore()
    for target in (left, right):
        pl.semaphore_signal(barrier, inc=1, device_id={"fs": target}, device_id_type=MESH)
    for hop in range(1, m):
        pl.semaphore_signal(
            barrier, inc=1, device_id={"tp": lax.rem(tp + hop, m)}, device_id_type=MESH
        )
    pl.semaphore_wait(barrier, 2 + m - 1)

    def columns(index, size):
        return pl.ds(pl.multiple_of(index * size, 128), size)

    def gather_far(phase, hop, source):
        return pltpu.make_async_remote_copy(
            src_ref=source,
            dst_ref=gathered.at[:, columns(tp, width)],
            send_sem=ag_far_send.at[phase, hop],
            recv_sem=ag_far_recv.at[phase, hop],
            device_id={"tp": lax.rem(tp + 2 * hop, m)},
            device_id_type=MESH,
        )

    def gather_near(phase, hop, source=None, arriving=False):
        origin = lax.rem((partner if arriving else tp) - 2 * hop + 2 * m, m)
        place = gathered.at[:, columns(origin, width)]
        return pltpu.make_async_remote_copy(
            src_ref=place if source is None else source,
            dst_ref=place,
            send_sem=ag_near_send.at[phase, hop],
            recv_sem=ag_near_recv.at[phase, hop],
            device_id={"tp": partner},
            device_id_type=MESH,
        )

    def gather_arrived_far(phase, hop):
        origin = lax.rem(tp - 2 * hop + 2 * m, m)
        place = gathered.at[:, columns(origin, width)]
        return pltpu.make_async_remote_copy(
            src_ref=place,
            dst_ref=place,
            send_sem=ag_far_send.at[phase, hop],
            recv_sem=ag_far_recv.at[phase, hop],
            device_id={"tp": origin},
            device_id_type=MESH,
        )

    def gather_start(phase, source):
        for hop in range(1, chips):
            gather_far(phase, hop, source).start()
        gather_near(phase, 0, source).start()

    def gather_forward(phase):
        for hop in range(1, chips):
            gather_arrived_far(phase, hop).wait_recv()
            gather_near(phase, hop).start()

    def gather_finish(phase, source):
        for hop in range(chips):
            gather_near(phase, hop, arriving=True).wait_recv()
            gather_near(phase, hop, source if hop == 0 else None).wait_send()
        for hop in range(1, chips):
            gather_far(phase, hop, source).wait_send()

    def normalise(gain):
        size = tile_of(rows, 64)

        @pl.loop(0, rows // size)
        def _(i):
            place = pl.ds(pl.multiple_of(i * size, size), size)
            values = gathered[place, :].astype(F32)
            scale = lax.rsqrt(jnp.mean(values * values, axis=-1, keepdims=True) + norm_eps)
            normed[place, :] = (values * scale * gain[...]).astype(BF16)

    row_tile = tile_of(rows, 256)
    unit_tile = tile_of(units, 256, 128)

    def hidden_part(gate, up, part, parts):
        count = rows // row_tile * (units // unit_tile) // parts
        across = units // unit_tile

        @pl.loop(part * count, (part + 1) * count)
        def _(i):
            place = pl.ds(pl.multiple_of((i // across) * row_tile, row_tile), row_tile)
            cols = columns(i % across, unit_tile)
            gate_value = dot(normed[place, :], gate[:, cols])
            up_value = dot(normed[place, :], up[:, cols])
            hidden[place, cols] = (jax.nn.silu(gate_value) * up_value).astype(BF16)

    def near_copy(phase, b):
        slot = b // q // 2 * q + b % q
        return pltpu.make_async_remote_copy(
            src_ref=terms.at[:, columns(b, block)],
            dst_ref=near.at[:, columns(slot, block)],
            send_sem=rs_near_send.at[phase, b],
            recv_sem=rs_near_recv.at[phase, slot],
            device_id={"tp": partner},
            device_id_type=MESH,
        )

    def far_copy(phase, b):
        to_chip = b // q // 2
        hop = lax.rem(to_chip - chip + chips, chips)
        slot = (hop - 1) * q + b % q
        return pltpu.make_async_remote_copy(
            src_ref=terms.at[:, columns(b, block)],
            dst_ref=far.at[:, columns(slot, block)],
            send_sem=rs_far_send.at[phase, b],
            recv_sem=rs_far_recv.at[phase, slot],
            device_id={"tp": to_chip * 2 + core},
            device_id_type=MESH,
        )

    def terms_of(phase, left_ref, weight, b):
        weights = pl.ds(pl.multiple_of(b * block, block), block)

        @pl.loop(0, rows // row_tile)
        def _(i):
            place = pl.ds(pl.multiple_of(i * row_tile, row_tile), row_tile)
            value = dot_last(left_ref[place, :], weight[weights, :])
            terms[place, columns(b, block)] = value.astype(BF16)

        @pl.when(b // q % 2 != core)
        def _():
            near_copy(phase, b).start()

    def pass_on(phase, b):
        mine = b // q % 2 == core
        slot = b // q // 2 * q + b % q

        @pl.when(mine)
        def _():
            near_copy(phase, b).wait_recv()

        @pl.when(mine & (b // q // 2 != chip))
        def _():
            @pl.loop(0, rows // row_tile)
            def _(i):
                place = pl.ds(pl.multiple_of(i * row_tile, row_tile), row_tile)
                total = terms[place, columns(b, block)].astype(F32)
                total = total + near[place, columns(slot, block)].astype(F32)
                terms[place, columns(b, block)] = total.astype(BF16)

            far_copy(phase, b).start()

    def blocks_at(step):
        if step == 0:
            return [fs]
        if step == h:
            return [owner(at + h)]
        return [owner(at - step), owner(at + step)]

    def far_arrived(phase, hop, k):
        slot = (hop - 1) * q + k
        place = far.at[:, slot * block : (slot + 1) * block]
        return pltpu.make_async_remote_copy(
            src_ref=place,
            dst_ref=place,
            send_sem=rs_far_send.at[phase, 0],
            recv_sem=rs_far_recv.at[phase, slot],
            device_id={"tp": partner},
            device_id_type=MESH,
        )

    def finish_sum(phase, factor, whole):
        for hop in range(1, chips):
            for k in range(q):
                far_arrived(phase, hop, k).wait_recv()

        @pl.loop(0, rows // row_tile)
        def _(i):
            place = pl.ds(pl.multiple_of(i * row_tile, row_tile), row_tile)
            total = terms[place, columns(tp, width)].astype(F32)
            total = total + near[place, columns(chip, width)].astype(F32)
            for hop in range(1, chips):
                total = total + far[place, (hop - 1) * width : hop * width].astype(F32)
            value = (stream[place, :].astype(F32) + factor * total).astype(BF16)
            stream[place, :] = value
            if whole:
                gathered[place, columns(tp, width)] = value

    def sent_sum(phase):
        for b in range(n):

            @pl.when(b // q % 2 != core)
            def _():
                near_copy(phase, b).wait_send()

            @pl.when((b // q % 2 == core) & (b // q // 2 != chip))
            def _():
                far_copy(phase, b).wait_send()

    gather_start(0, tokens)
    launch(G1, U1)
    own = [
        pltpu.make_async_copy(tokens, stream, own_sem.at[0]),
        pltpu.make_async_copy(tokens, gathered.at[:, columns(tp, width)], own_sem.at[1]),
    ]
    mine = pl.ds(pl.multiple_of(fs * block, block), block)
    for k in range(9):
        source, buffer, _, _ = plan[k]
        own.append(pltpu.make_async_copy(source, buffer.at[mine], own_sem.at[2 + k]))
    for copy in own:
        copy.start()
    rate_map[...] = jnp.zeros_like(rate_map)
    input_map[...] = jnp.zeros_like(input_map)
    for k in range(lanes // HEAD_DIM):
        part = slice(k * HEAD_DIM, (k + 1) * HEAD_DIM)
        rate_map[part, part] = rate_weight[k]
        input_map[part, part] = input_weight[k]
    lane[0:8, :] = jnp.zeros((8, lanes), F32)
    for copy in own:
        copy.wait()

    serve(G1, 1)
    gather_forward(0)
    serve(U1, 1)
    gather_finish(0, tokens)
    normalise(first_gain)
    for step in range(2, h + 1):
        serve(G1, step)
        serve(U1, step)
        if step == h - 1:
            launch(D1)
    launch(MI, MB, MO)
    hidden_part(w_gate1, w_up1, 0, 1)
    for b in blocks_at(0):
        terms_of(0, hidden, w_down1, b)
    for step in range(1, h + 1):
        serve(D1, step)
        for b in blocks_at(step):
            terms_of(0, hidden, w_down1, b)
        for k in (MI, MB, MO):
            serve(k, step)
        for b in blocks_at(step - 1):
            pass_on(0, b)
        if step == h - 1:
            launch(G2, U2)
    for b in blocks_at(h):
        pass_on(0, b)
    finish_sum(0, 0.5, True)
    gather_start(1, stream)
    sent_sum(0)

    queue = [(k, step) for step in range(1, h + 1) for k in (G2, U2)]

    def take(count):
        for _ in range(min(count, len(queue))):
            k, step = queue.pop(0)
            serve(k, step)
            if k == U2 and step == h - 1:
                launch(D2A, D2B)

    take(1)
    gather_forward(1)
    take(1)
    gather_finish(1, stream)
    normalise(mix_gain)

    @pl.loop(0, rows // row_tile)
    def _(i):
        place = pl.ds(pl.multiple_of(i * row_tile, row_tile), row_tile)
        lower = pl.ds(pl.multiple_of(i * row_tile + 8, 8), row_tile)
        value = dot(normed[place, :], w_in[...])
        lane[lower, :] = value.astype(BF16).astype(F32)
        branch[place, :] = dot(normed[place, :], w_branch[...])

    slope = -rate_scale * jnp.log1p(jnp.exp(-decay_param[...]))
    small = tile_of(rows, 128)
    lane_id = lax.broadcasted_iota(jnp.int32, (small, lanes), 1) // HEAD_DIM

    @pl.loop(0, rows // small)
    def _(i):
        place = pl.ds(pl.multiple_of(i * small, small), small)
        upper = lane[pl.ds(pl.multiple_of(i * small, 8), small + 8), :]
        conv_sum = jnp.zeros((small, lanes), F32)
        for k in range(CONV):
            shifted = pltpu.roll(upper, CONV - 1 - k, 0) if k < CONV - 1 else upper
            conv_sum = conv_sum + shifted[8:, :] * conv_weight[k : k + 1, :].astype(F32)
        conv_out = conv_sum.astype(BF16)
        rate = jax.nn.sigmoid(dot(conv_out, rate_map[...]))
        admit = jax.nn.sigmoid(dot(conv_out, input_map[...]))
        shifts = decay_shift[place, :]
        shift = jnp.zeros((small, lanes), F32)
        for k in range(lanes // HEAD_DIM):
            shift = jnp.where(lane_id == k, shifts[:, k : k + 1], shift)
        log_decay = rate * slope + shift
        decay[place, :] = jnp.exp(log_decay)
        drive[place, :] = (
            jnp.sqrt(negative_expm1(2.0 * log_decay)) * admit * conv_out.astype(F32)
        )

    take(1)
    lane_tile = tile_of(lanes, 128)
    row_id = lax.broadcasted_iota(jnp.int32, (rows, lane_tile), 0)

    @pl.loop(0, lanes // lane_tile)
    def _(i):
        cols = columns(i, lane_tile)
        factor, state = decay[:, cols], drive[:, cols]
        reach = 1
        while reach < rows:
            inside = row_id >= reach
            state = factor * jnp.where(inside, pltpu.roll(state, reach, 0), 0.0) + state
            if reach * 2 < rows:
                factor = factor * jnp.where(inside, pltpu.roll(factor, reach, 0), 1.0)
            reach *= 2
        mixed[:, cols] = (state * jax.nn.gelu(branch[:, cols])).astype(BF16)

    take(1)
    for step in range(h + 1):
        for b in blocks_at(step):
            terms_of(1, mixed, w_out, b)
        if step:
            for b in blocks_at(step - 1):
                pass_on(1, b)
    for b in blocks_at(h):
        pass_on(1, b)
    take(1)
    finish_sum(1, 1.0, True)
    gather_start(2, stream)
    sent_sum(1)
    take(1)
    gather_forward(2)
    take(2 * h)
    gather_finish(2, stream)

    normalise(second_gain)
    halves = [(k, step) for step in range(1, h + 1) for k in (D2A, D2B)]
    parts = tile_of(rows // row_tile, 4, 2)
    for part in range(parts):
        serve(*halves.pop(0))
        hidden_part(w_gate2, w_up2, part, parts)
    for b in blocks_at(0):
        terms_of(2, hidden, w_down2, b)
    for step in range(1, h + 1):
        while halves and halves[0][1] <= step:
            serve(*halves.pop(0))
        for b in blocks_at(step):
            terms_of(2, hidden, w_down2, b)
        for b in blocks_at(step - 1):
            pass_on(2, b)
    for b in blocks_at(h):
        pass_on(2, b)
    finish_sum(2, 0.5, False)

    @pl.loop(0, rows // row_tile)
    def _(i):
        place = pl.ds(pl.multiple_of(i * row_tile, row_tile), row_tile)
        values = stream[place, :].astype(F32)
        squares = jnp.sum(values * values, axis=-1, keepdims=True)
        square_own[:, columns(i, row_tile)] = jnp.broadcast_to(squares, (row_tile, 128)).T[:8, :]

    def square_copy(hop):
        return pltpu.make_async_remote_copy(
            src_ref=square_own,
            dst_ref=square_in.at[hop - 1],
            send_sem=sq_send.at[hop],
            recv_sem=sq_recv.at[hop],
            device_id={"tp": lax.rem(tp + hop, m)},
            device_id_type=MESH,
        )

    for hop in range(1, m):
        square_copy(hop).start()
    sent_sum(2)
    for k in range(len(plan)):
        for way in (0, 1):
            for step in range(h):
                ring_copy(k, way, step).wait_send()
    for hop in range(1, m):
        square_copy(hop).wait()

    @pl.loop(0, rows // row_tile)
    def _(i):
        place = pl.ds(pl.multiple_of(i * row_tile, row_tile), row_tile)
        cols = columns(i, row_tile)
        squares = square_own[:, cols]
        for hop in range(1, m):
            squares = squares + square_in[hop - 1, :, cols]
        spread = jnp.broadcast_to(squares[0:1, :], (128, row_tile)).T
        scale_out[place, :] = lax.rsqrt(spread / d + norm_eps)


def shards(n, m, *arrays):
    (
        tokens,
        first_gain,
        first_gate,
        first_up,
        first_down,
        mix_gain,
        mix_input,
        mix_branch,
        conv_weight,
        rate_weight,
        input_weight,
        decay_param,
        decay_shift,
        mix_output,
        second_gain,
        second_gate,
        second_up,
        second_down,
        final_gain,
    ) = arrays
    rows, width = tokens.shape
    d = width * m
    units = first_gate.shape[1]
    lanes = mix_input.shape[1]
    h, q, chips = n // 2, n // m, m // 2
    hbm = pl.BlockSpec(memory_space=pl.ANY)
    vmem = pl.BlockSpec(memory_space=pltpu.VMEM)
    dma = pltpu.SemaphoreType.DMA
    stream, scale = pl.pallas_call(
        functools.partial(kernel, n, m),
        out_shape=(
            jax.ShapeDtypeStruct((rows, width), BF16),
            jax.ShapeDtypeStruct((rows, 128), F32),
        ),
        in_specs=[hbm] * 10 + [vmem] * 8,
        out_specs=(vmem, vmem),
        scratch_shapes=[
            *[pltpu.VMEM((d, units), BF16)] * 3,
            *[pltpu.VMEM((d, lanes), BF16)] * 3,
            *[pltpu.VMEM((d, units), BF16)] * 3,
            pltpu.VMEM((rows, d), BF16),
            pltpu.VMEM((rows, d), BF16),
            pltpu.VMEM((rows, units), BF16),
            pltpu.VMEM((rows, d), BF16),
            pltpu.VMEM((rows, chips * width), BF16),
            pltpu.VMEM((rows, max(chips - 1, 1) * width), BF16),
            pltpu.VMEM((rows, lanes), BF16),
            pltpu.VMEM((rows + 8, lanes), F32),
            pltpu.VMEM((rows, lanes), F32),
            pltpu.VMEM((rows, lanes), F32),
            pltpu.VMEM((rows, lanes), F32),
            pltpu.VMEM((lanes, lanes), BF16),
            pltpu.VMEM((lanes, lanes), BF16),
            pltpu.VMEM((8, rows), F32),
            pltpu.VMEM((m - 1, 8, rows), F32),
            dma((10, 2, h)),
            dma((10, 2, h)),
            dma((11,)),
            dma((3, chips)),
            dma((3, chips)),
            dma((3, chips)),
            dma((3, chips)),
            dma((3, n)),
            dma((3, n // 2)),
            dma((3, n)),
            dma((3, max(chips - 1, 1) * q)),
            dma((m,)),
            dma((m,)),
        ],
        compiler_params=pltpu.CompilerParams(
            collective_id=0, has_side_effects=True, vmem_limit_bytes=67043328
        ),
        cost_estimate=pl.CostEstimate(
            flops=rows * d * (12 * units + 6 * lanes), bytes_accessed=8 * d * units, transcendentals=0
        ),
    )(
        tokens,
        first_gate,
        first_up,
        first_down,
        mix_input,
        mix_branch,
        mix_output,
        second_gate,
        second_up,
        second_down,
        first_gain[None, :],
        mix_gain[None, :],
        second_gain[None, :],
        conv_weight,
        rate_weight,
        input_weight,
        decay_param[None, :],
        decay_shift,
    )
    return (stream.astype(F32) * scale[:, :1] * final_gain).astype(BF16)


def solution(mesh):
    return jax.shard_map(
        functools.partial(shards, mesh.shape["fs"], mesh.shape["tp"]),
        mesh=mesh,
        in_specs=(
            P("fs", "tp"),
            P(),
            P("fs", "tp"),
            P("fs", "tp"),
            P("fs", "tp"),
            P(),
            P("fs", "tp"),
            P("fs", "tp"),
            P(None, "tp"),
            P("tp", None, None),
            P("tp", None, None),
            P("tp"),
            P("fs", "tp"),
            P("fs", "tp"),
            P(),
            P("fs", "tp"),
            P("fs", "tp"),
            P("fs", "tp"),
            P("tp"),
        ),
        out_specs=P("fs", "tp"),
        check_vma=False,
    )
```

```python
import functools

import jax
import jax.numpy as jnp
from jax import lax
from jax.experimental import pallas as pl
from jax.experimental.pallas import tpu as pltpu
from jax.sharding import PartitionSpec as P

HEAD_DIM = 64
CONV = 4
norm_eps = 1e-06
rate_scale = 8.0
MESH = pl.DeviceIdType.MESH
F32, BF16 = jnp.float32, jnp.bfloat16
G1, U1, D1, MI, MB, MO, G2, U2, D2A, D2B = range(10)


def tile_of(size, *choices):
    for choice in choices:
        if size % choice == 0:
            return choice
    return size


def negative_expm1(y):
    series = 1.0 + y * (1.0 / 6.0)
    for k in (5, 4, 3, 2):
        series = 1.0 + y * (1.0 / k) * series
    return jnp.where(y > -0.25, -y * series, 1.0 - jnp.exp(y))


def scoped(f):
    def g(*args):
        tag = "_".join(str(a) for a in args if isinstance(a, int))
        with jax.named_scope(f"{f.__name__}_{tag}"):
            return f(*args)

    return g


def dot(left, right):
    return jnp.dot(left, right, preferred_element_type=F32)


def dot_last(left, right):
    return lax.dot_general(left, right, (((1,), (1,)), ((), ())), preferred_element_type=F32)


def kernel(
    n,
    m,
    split,
    tokens,
    first_gate,
    first_up,
    first_down,
    mix_input,
    mix_branch,
    mix_output,
    second_gate,
    second_up,
    second_down,
    first_gain,
    mix_gain,
    second_gain,
    conv_weight,
    rate_weight,
    input_weight,
    decay_param,
    decay_shift,
    final_gain,
    stream,
    w_gate1,
    w_up1,
    w_down1,
    w_in,
    w_branch,
    w_out,
    w_gate2,
    w_up2,
    w_down2,
    gathered,
    gathered_mate,
    normed,
    normed_mate,
    hidden,
    hidden_half,
    near,
    near_mate,
    far,
    far_mate,
    from_mate,
    mixed,
    lane,
    branch,
    decay,
    drive,
    rate_map,
    input_map,
    square_own,
    square_in,
    ring_send,
    ring_recv,
    own_sem,
    ag_near_send,
    ag_near_recv,
    ag_far_send,
    ag_far_recv,
    rs_near_send,
    rs_near_recv,
    rs_far_send,
    rs_far_recv,
    sq_send,
    sq_recv,
    spread_send,
    spread_recv,
    cross_send,
    cross_recv,
    mate_send,
    mate_recv,
):
    h = n // 2
    chips = m // 2
    q = n // m
    rows, width = stream.shape
    d = width * m
    block = d // n
    units = first_gate.shape[1]
    lanes = mix_input.shape[1]
    fs = lax.axis_index("fs")
    tp = lax.axis_index("tp")
    chip = tp // 2
    core = tp % 2
    partner = tp + 1 - 2 * core
    at = jnp.where(fs % 2 == 0, fs // 2, n - 1 - fs // 2)

    def owner(place):
        p = lax.rem(place + 2 * n, n)
        return jnp.where(p < h, 2 * p, 2 * (n - 1 - p) + 1)

    right, left = owner(at + 1), owner(at - 1)
    part_units = w_gate1.shape[1]
    places = n // 2
    line, side = fs // 2, fs % 2

    def flip(value, bits):
        bit = 1
        while bit <= bits:
            if bits & bit:
                value = value + bit - 2 * bit * (value // bit % 2)
            bit *= 2
        return value

    def share(place):
        return (place % 4 + 1) // 2 % 2

    mate = flip(line, 1) * 2 + side
    half = block // 2
    plan = [
        (first_gate, w_gate1, 0, block),
        (first_up, w_up1, 0, block),
        (first_down, w_down1, 0, block),
        (mix_input, w_in, 0, block),
        (mix_branch, w_branch, 0, block),
        (mix_output, w_out, 0, block),
        (second_gate, w_gate2, 0, block),
        (second_up, w_up2, 0, block),
        (second_down, w_down2, 0, half),
        (second_down, w_down2, half, half),
    ]

    def ring_copy(k, way, step, arriving=False):
        source, buffer, low, count = plan[k]
        sign = -1 if way == 0 else 1
        b = owner(at + sign * (step + 1 if arriving else step))
        if step == h - 1:
            count = count // 2
            low = low + way * count
        place = pl.ds(pl.multiple_of(b * block + low, 16), count)
        if step == 0 and not arriving:
            src = source if count == block else source.at[pl.ds(low, count)]
        else:
            src = buffer.at[place]
        return pltpu.make_async_remote_copy(
            src_ref=src,
            dst_ref=buffer.at[place],
            send_sem=ring_send.at[k, way, step],
            recv_sem=ring_recv.at[k, way, step],
            device_id={"fs": right if way == 0 else left},
            device_id_type=MESH,
        )

    @scoped
    def launch(*ks):
        for k in ks:
            for way in (0, 1):
                ring_copy(k, way, 0).start()

    @scoped
    def serve(k, step):
        for way in (0, 1):
            ring_copy(k, way, step - 1, arriving=True).wait_recv()
            if step < h:
                ring_copy(k, way, step).start()

    barrier = pltpu.get_barrier_semaphore()
    for hop in range(1, n):
        pl.semaphore_signal(
            barrier, inc=1, device_id={"fs": lax.rem(fs + hop, n)}, device_id_type=MESH
        )
    for hop in range(1, m):
        pl.semaphore_signal(
            barrier, inc=1, device_id={"tp": lax.rem(tp + hop, m)}, device_id_type=MESH
        )
    pl.semaphore_wait(barrier, n - 1 + m - 1)

    def columns(index, size):
        return pl.ds(pl.multiple_of(index * size, 128), size)

    def full_of(phase):
        return gathered_mate if phase == 3 else gathered

    def terms_ref(phase):
        return normed_mate if phase == 3 else normed

    def near_of(phase):
        return near_mate if phase == 3 else near

    def far_of(phase):
        return far_mate if phase == 3 else far

    def gather_far(phase, hop, source):
        return pltpu.make_async_remote_copy(
            src_ref=source,
            dst_ref=full_of(phase).at[:, columns(tp, width)],
            send_sem=ag_far_send.at[phase, hop],
            recv_sem=ag_far_recv.at[phase, hop],
            device_id={"tp": lax.rem(tp + 2 * hop, m)},
            device_id_type=MESH,
        )

    def gather_near(phase, hop, source=None, arriving=False):
        origin = lax.rem((partner if arriving else tp) - 2 * hop + 2 * m, m)
        place = full_of(phase).at[:, columns(origin, width)]
        return pltpu.make_async_remote_copy(
            src_ref=place if source is None else source,
            dst_ref=place,
            send_sem=ag_near_send.at[phase, hop],
            recv_sem=ag_near_recv.at[phase, hop],
            device_id={"tp": partner},
            device_id_type=MESH,
        )

    def gather_arrived_far(phase, hop):
        origin = lax.rem(tp - 2 * hop + 2 * m, m)
        place = full_of(phase).at[:, columns(origin, width)]
        return pltpu.make_async_remote_copy(
            src_ref=place,
            dst_ref=place,
            send_sem=ag_far_send.at[phase, hop],
            recv_sem=ag_far_recv.at[phase, hop],
            device_id={"tp": origin},
            device_id_type=MESH,
        )

    @scoped
    def gather_start(phase, source):
        for hop in range(1, chips):
            gather_far(phase, hop, source).start()
        gather_near(phase, 0, source).start()

    @scoped
    def gather_forward(phase):
        for hop in range(1, chips):
            gather_arrived_far(phase, hop).wait_recv()
            gather_near(phase, hop).start()

    @scoped
    def gather_finish(phase, source):
        for hop in range(chips):
            gather_near(phase, hop, arriving=True).wait_recv()
            gather_near(phase, hop, source if hop == 0 else None).wait_send()
        for hop in range(1, chips):
            gather_far(phase, hop, source).wait_send()

    @scoped
    def normalise(gain, phase=0):
        size = tile_of(rows, 64)

        @pl.loop(0, rows // size)
        def _(i):
            place = pl.ds(pl.multiple_of(i * size, size), size)
            values = full_of(phase)[place, :].astype(F32)
            scale = lax.rsqrt(jnp.mean(values * values, axis=-1, keepdims=True) + norm_eps)
            terms_ref(phase)[place, :] = (values * scale * gain[...]).astype(BF16)

    row_tile = tile_of(rows, 256)

    def hidden_view(size):
        return hidden if size == hidden.shape[1] else hidden_half

    @scoped
    def hidden_part(gate, up, part, parts, phase=2):
        size = gate.shape[1]
        unit_tile = tile_of(size, 256, 640, 128)
        across = size // unit_tile
        count = rows // row_tile * across // parts
        first = rows if phase == 3 else 0
        source = terms_ref(phase)
        goal = hidden_view(size)

        @pl.loop(part * count, (part + 1) * count)
        def _(i):
            start = pl.multiple_of((i // across) * row_tile, row_tile)
            place = pl.ds(start, row_tile)
            cols = columns(i % across, unit_tile)
            gate_value = dot(source[place, :], gate[:, cols])
            up_value = dot(source[place, :], up[:, cols])
            goal[pl.ds(start + first, row_tile), cols] = (
                jax.nn.silu(gate_value) * up_value
            ).astype(BF16)

    def grain(phase):
        return half if phase == 2 and half % 128 == 0 else block

    def pieces(phase):
        return width // grain(phase)

    def near_copy(phase, b):
        q, block = pieces(phase), grain(phase)
        slot = b // q // 2 * q + b % q
        return pltpu.make_async_remote_copy(
            src_ref=terms_ref(phase).at[:, columns(b, block)],
            dst_ref=near_of(phase).at[:, columns(slot, block)],
            send_sem=rs_near_send.at[phase, b],
            recv_sem=rs_near_recv.at[phase, slot],
            device_id={"tp": partner},
            device_id_type=MESH,
        )

    def far_copy(phase, b):
        q, block = pieces(phase), grain(phase)
        to_chip = b // q // 2
        hop = lax.rem(to_chip - chip + chips, chips)
        slot = (hop - 1) * q + b % q
        return pltpu.make_async_remote_copy(
            src_ref=terms_ref(phase).at[:, columns(b, block)],
            dst_ref=far_of(phase).at[:, columns(slot, block)],
            send_sem=rs_far_send.at[phase, b],
            recv_sem=rs_far_recv.at[phase, slot],
            device_id={"tp": to_chip * 2 + core},
            device_id_type=MESH,
        )

    @scoped
    def terms_of(phase, left_ref, weight, b):
        q, block = pieces(phase), grain(phase)
        first = rows if phase == 3 else 0
        tall = tile_of(rows, 512)
        weights = pl.ds(pl.multiple_of(b * block, block), block)

        @pl.loop(0, rows // tall)
        def _(i):
            place = pl.ds(pl.multiple_of(i * tall, tall), tall)
            inner = pl.ds(pl.multiple_of(i * tall + first, tall), tall)
            value = dot_last(left_ref[inner, :], weight[weights, :])
            terms_ref(phase)[place, columns(b, block)] = value.astype(BF16)

        @pl.when(b // q % 2 != core)
        def _():
            near_copy(phase, b).start()

    @scoped
    def pass_on(phase, b):
        q, block = pieces(phase), grain(phase)
        mine = b // q % 2 == core
        slot = b // q // 2 * q + b % q

        @pl.when(mine)
        def _():
            near_copy(phase, b).wait_recv()

        @pl.when(mine & (b // q // 2 != chip))
        def _():
            @pl.loop(0, rows // row_tile)
            def _(i):
                place = pl.ds(pl.multiple_of(i * row_tile, row_tile), row_tile)
                total = terms_ref(phase)[place, columns(b, block)].astype(F32)
                total = total + near_of(phase)[place, columns(slot, block)].astype(F32)
                terms_ref(phase)[place, columns(b, block)] = total.astype(BF16)

            far_copy(phase, b).start()

    def blocks_at(step):
        if step == 0:
            return [fs]
        if step == h:
            return [owner(at + h)]
        return [owner(at - step), owner(at + step)]

    def far_arrived(phase, hop, k):
        q, block = pieces(phase), grain(phase)
        slot = (hop - 1) * q + k
        place = far_of(phase).at[:, slot * block : (slot + 1) * block]
        return pltpu.make_async_remote_copy(
            src_ref=place,
            dst_ref=place,
            send_sem=rs_far_send.at[phase, 0],
            recv_sem=rs_far_recv.at[phase, slot],
            device_id={"tp": partner},
            device_id_type=MESH,
        )

    def sum_of(phase, place):
        total = terms_ref(phase)[place, columns(tp, width)].astype(F32)
        total = total + near_of(phase)[place, columns(chip, width)].astype(F32)
        for hop in range(1, chips):
            total = total + far_of(phase)[place, (hop - 1) * width : hop * width].astype(F32)
        return total

    def mate_copy(which):
        cols = columns(tp, width)
        return pltpu.make_async_remote_copy(
            src_ref=normed_mate.at[:, cols] if which else tokens,
            dst_ref=from_mate if which else gathered_mate.at[:, cols],
            send_sem=mate_send.at[which],
            recv_sem=mate_recv.at[which],
            device_id={"fs": mate},
            device_id_type=MESH,
        )

    @scoped
    def finish_mate():
        for hop in range(1, chips):
            for k in range(pieces(3)):
                far_arrived(3, hop, k).wait_recv()

        @pl.loop(0, rows // row_tile)
        def _(i):
            place = pl.ds(pl.multiple_of(i * row_tile, row_tile), row_tile)
            normed_mate[place, columns(tp, width)] = sum_of(3, place).astype(BF16)

        mate_copy(1).start()

    @scoped
    def finish_sum(phase, factor, whole):
        for hop in range(1, chips):
            for k in range(pieces(phase)):
                far_arrived(phase, hop, k).wait_recv()
        if phase == 0 and split:
            mate_copy(1).wait_recv()
            launch(G2, U2)

        @pl.loop(0, rows // row_tile)
        def _(i):
            place = pl.ds(pl.multiple_of(i * row_tile, row_tile), row_tile)
            total = sum_of(phase, place)
            if phase == 0 and split:
                total = total + from_mate[place, :].astype(F32)
            value = (stream[place, :].astype(F32) + factor * total).astype(BF16)
            stream[place, :] = value
            if whole:
                gathered[place, columns(tp, width)] = value

    @scoped
    def sent_sum(phase):
        q = pieces(phase)
        for b in range(q * m):

            @pl.when(b // q % 2 != core)
            def _():
                near_copy(phase, b).wait_send()

            @pl.when((b // q % 2 == core) & (b // q // 2 != chip))
            def _():
                far_copy(phase, b).wait_send()

    def part_rows(place, beside, low):
        return pl.ds(pl.multiple_of((place * 2 + beside) * block + low, 16), half)

    def own_part(k, place):
        low = k % 2 * half
        return plan[k // 2][0].at[low : low + half, columns(share(place), part_units)]

    def spread_copy(k, bits):
        other = flip(line, bits)
        return pltpu.make_async_remote_copy(
            src_ref=own_part(k, other),
            dst_ref=plan[k // 2][1].at[part_rows(line, side, k % 2 * half)],
            send_sem=spread_send.at[k, bits],
            recv_sem=spread_recv.at[k, bits],
            device_id={"fs": other * 2 + side},
            device_id_type=MESH,
        )

    def spread_arrived(k, bits):
        place = plan[k // 2][1].at[part_rows(flip(line, bits), side, k % 2 * half)]
        return pltpu.make_async_remote_copy(
            src_ref=place,
            dst_ref=place,
            send_sem=spread_send.at[k, bits],
            recv_sem=spread_recv.at[k, bits],
            device_id={"fs": mate},
            device_id_type=MESH,
        )

    def cross_copy(k, bits, arriving=False):
        beside = 1 - side if arriving else side
        place = plan[k // 2][1].at[part_rows(flip(line, bits), beside, k % 2 * half)]
        return pltpu.make_async_remote_copy(
            src_ref=own_part(k, line) if bits == 0 and not arriving else place,
            dst_ref=place,
            send_sem=cross_send.at[k, bits],
            recv_sem=cross_recv.at[k, bits],
            device_id={"fs": fs + 1 - 2 * side},
            device_id_type=MESH,
        )

    last_first = [*range(2, places), 1]

    @scoped
    def cross(k):
        for bits in last_first:
            spread_arrived(k, bits).wait_recv()
            cross_copy(k, bits).start()
            spread_copy(k, bits).wait_send()
            if k + 2 < 6:
                spread_copy(k + 2, bits).start()

    @scoped
    def crossed(k):
        for part in (2 * k, 2 * k + 1):
            for bits in range(places):
                cross_copy(part, bits, arriving=True).wait_recv()

    if split:
        for bits in range(1, places):
            spread_copy(0, bits).start()
        for k in range(6):
            cross_copy(k, 0).start()
    else:
        launch(G1, U1)
    gather_start(0, tokens)
    own = [
        pltpu.make_async_copy(tokens, stream, own_sem.at[0]),
        pltpu.make_async_copy(tokens, gathered.at[:, columns(tp, width)], own_sem.at[1]),
    ]
    mine = pl.ds(pl.multiple_of(fs * block, block), block)
    for k in range(9):
        source, buffer, _, _ = plan[k]
        if split and k in (G1, U1, D1):
            source = source.at[:, columns(share(line), part_units)]
        own.append(pltpu.make_async_copy(source, buffer.at[mine], own_sem.at[2 + k]))
    for copy in own:
        copy.start()
    rate_map[...] = jnp.zeros_like(rate_map)
    input_map[...] = jnp.zeros_like(input_map)
    for k in range(lanes // HEAD_DIM):
        part = slice(k * HEAD_DIM, (k + 1) * HEAD_DIM)
        rate_map[part, part] = rate_weight[k]
        input_map[part, part] = input_weight[k]
    lane[0:8, :] = jnp.zeros((8, lanes), F32)
    with jax.named_scope("ownwait"):
        for copy in own:
            copy.wait()

    if split:
        own_cols = gathered_mate.at[:, columns(tp, width)]
        mixes = [(k, step) for step in range(1, h + 1) for k in (MI, MB, MO)]

        def mix_serve(count):
            for _ in range(min(count, len(mixes))):
                serve(*mixes.pop(0))

        for bits in range(1, places):
            spread_copy(1, bits).start()
        cross(0)
        mate_copy(0).start()
        gather_forward(0)
        cross(1)
        gather_finish(0, tokens)
        normalise(first_gain)
        cross(2)
        with jax.named_scope("matewait"):
            mate_copy(0).wait_recv()
        gather_start(3, own_cols)
        cross(3)
        cross(4)
        gather_forward(3)
        cross(5)
        gather_finish(3, own_cols)
        normalise(first_gain, 3)
        crossed(G1)
        crossed(U1)
        parts = tile_of(rows // row_tile, 4, 2)
        launch(MI, MB, MO)
        hidden_part(w_gate1, w_up1, 0, 1, 3)
        crossed(D1)
        for b in range(n):
            terms_of(3, hidden_half, w_down1, b)
            if b:
                pass_on(3, b - 1)
        pass_on(3, n - 1)
        mix_serve(3)
        for part in range(parts):
            hidden_part(w_gate1, w_up1, part, parts, 0)
            if part == 1:
                mix_serve(3)
        mix_serve(3)
        finish_mate()
        mix_serve(len(mixes))
        for b in range(n):
            terms_of(0, hidden_half, w_down1, b)
            if b:
                pass_on(0, b - 1)
        pass_on(0, n - 1)
    else:
        serve(G1, 1)
        gather_forward(0)
        serve(U1, 1)
        gather_finish(0, tokens)
        normalise(first_gain)
        for step in range(2, h + 1):
            serve(G1, step)
            serve(U1, step)
            if step == h - 1:
                launch(D1)
        launch(MI, MB, MO)
        hidden_part(w_gate1, w_up1, 0, 1, 0)
        for b in blocks_at(0):
            terms_of(0, hidden, w_down1, b)
        for step in range(1, h + 1):
            serve(D1, step)
            for b in blocks_at(step):
                terms_of(0, hidden, w_down1, b)
            for k in (MI, MB, MO):
                serve(k, step)
            for b in blocks_at(step - 1):
                pass_on(0, b)
            if step == h - 1:
                launch(G2, U2)
        for b in blocks_at(h):
            pass_on(0, b)
    finish_sum(0, 0.5, True)
    gather_start(1, stream)
    sent_sum(0)
    if split:
        sent_sum(3)

    queue = [(k, step) for step in range(1, h + 1) for k in (G2, U2)]

    def take(count):
        for _ in range(min(count, len(queue))):
            k, step = queue.pop(0)
            serve(k, step)
            if k == U2 and step == h - 1:
                launch(D2A, D2B)

    take(1)
    gather_forward(1)
    gather_finish(1, stream)
    normalise(mix_gain)

    @pl.loop(0, rows // row_tile)
    def _(i):
        place = pl.ds(pl.multiple_of(i * row_tile, row_tile), row_tile)
        lower = pl.ds(pl.multiple_of(i * row_tile + 8, 8), row_tile)
        value = dot(normed[place, :], w_in[...])
        lane[lower, :] = value.astype(BF16).astype(F32)
        branch[place, :] = dot(normed[place, :], w_branch[...])

    slope = -rate_scale * jnp.log1p(jnp.exp(-decay_param[...]))
    small = tile_of(rows, 128)

    @pl.loop(0, rows // small)
    def _(i):
        place = pl.ds(pl.multiple_of(i * small, small), small)
        upper = lane[pl.ds(pl.multiple_of(i * small, 8), small + 8), :]
        conv_sum = jnp.zeros((small, lanes), F32)
        for k in range(CONV):
            shifted = pltpu.roll(upper, CONV - 1 - k, 0) if k < CONV - 1 else upper
            conv_sum = conv_sum + shifted[8:, :] * conv_weight[k : k + 1, :].astype(F32)
        conv_out = conv_sum.astype(BF16)
        rate = jax.nn.sigmoid(dot(conv_out, rate_map[...]))
        admit = jax.nn.sigmoid(dot(conv_out, input_map[...]))
        shifts = decay_shift[:, columns(i, small)]
        shift = jnp.concatenate(
            [
                jnp.broadcast_to(shifts[k : k + 1, :], (HEAD_DIM, small))
                for k in range(lanes // HEAD_DIM)
            ],
            axis=0,
        ).T
        log_decay = rate * slope + shift
        decay[place, :] = jnp.exp(log_decay)
        drive[place, :] = (
            jnp.sqrt(negative_expm1(2.0 * log_decay)) * admit * conv_out.astype(F32)
        )

    lane_tile = tile_of(lanes, 128)
    row_id = lax.broadcasted_iota(jnp.int32, (rows, lane_tile), 0)

    @pl.loop(0, lanes // lane_tile)
    def _(i):
        cols = columns(i, lane_tile)
        factor, state = decay[:, cols], drive[:, cols]
        reach = 1
        while reach < rows:
            inside = row_id >= reach
            state = factor * jnp.where(inside, pltpu.roll(state, reach, 0), 0.0) + state
            if reach * 2 < rows:
                factor = factor * jnp.where(inside, pltpu.roll(factor, reach, 0), 1.0)
            reach *= 2
        mixed[:, cols] = (state * jax.nn.gelu(branch[:, cols])).astype(BF16)

    take(1)
    for b in range(n):
        terms_of(1, mixed, w_out, b)
        if b:
            pass_on(1, b - 1)
    pass_on(1, n - 1)
    take(1)
    finish_sum(1, 1.0, True)
    gather_start(2, stream)
    sent_sum(1)
    take(3)
    gather_forward(2)
    take(2 * h - 1 - 6)
    gather_finish(2, stream)
    normalise(second_gain)
    take(2 * h)

    halves = [(k, step) for step in range(1, h + 1) for k in (D2A, D2B)]
    parts = tile_of(rows // row_tile, 4, 2)
    for part in range(parts):
        hidden_part(w_gate2, w_up2, part, parts)
        if part % 2 or parts < 4:
            serve(*halves.pop(0))
    fine = block // grain(2)
    for step in range(h + 1):
        for piece in range(2):
            while halves and (halves[0][1], halves[0][0]) <= (step, D2A + piece):
                serve(*halves.pop(0))
            if fine == 1 and piece == 0:
                continue
            fresh = [
                b * fine + e for b in blocks_at(step) for e in ([piece] if fine == 2 else [0])
            ]
            for b in fresh:
                terms_of(2, hidden, w_down2, b)
            for b in fresh:
                pass_on(2, b)
    finish_sum(2, 0.5, False)

    @pl.loop(0, rows // row_tile)
    def _(i):
        place = pl.ds(pl.multiple_of(i * row_tile, row_tile), row_tile)
        values = stream[place, :].astype(F32)
        squares = jnp.sum(values * values, axis=-1, keepdims=True)
        square_own[:, columns(i, row_tile)] = jnp.broadcast_to(squares, (row_tile, 128)).T[:8, :]

    def square_copy(hop):
        return pltpu.make_async_remote_copy(
            src_ref=square_own,
            dst_ref=square_in.at[hop - 1],
            send_sem=sq_send.at[hop],
            recv_sem=sq_recv.at[hop],
            device_id={"tp": lax.rem(tp + hop, m)},
            device_id_type=MESH,
        )

    for hop in range(1, m):
        square_copy(hop).start()
    sent_sum(2)
    for k in range(MI if split else 0, len(plan)):
        for way in (0, 1):
            for step in range(h):
                ring_copy(k, way, step).wait_send()
    if split:
        for k in range(6):
            for bits in range(places):
                cross_copy(k, bits).wait_send()
        for which in range(2):
            mate_copy(which).wait_send()
    with jax.named_scope("sqwait"):
        for hop in range(1, m):
            square_copy(hop).wait()

    @pl.loop(0, rows // row_tile)
    def _(i):
        place = pl.ds(pl.multiple_of(i * row_tile, row_tile), row_tile)
        cols = columns(i, row_tile)
        squares = square_own[:, cols]
        for hop in range(1, m):
            squares = squares + square_in[hop - 1, :, cols]
        spread = jnp.broadcast_to(squares[0:1, :], (128, row_tile)).T
        scale = lax.rsqrt(spread[:, 0:1] / d + norm_eps)
        stream[place, :] = (stream[place, :].astype(F32) * scale * final_gain[...]).astype(BF16)


def shards(n, m, *arrays):
    (
        tokens,
        first_gain,
        first_gate,
        first_up,
        first_down,
        mix_gain,
        mix_input,
        mix_branch,
        conv_weight,
        rate_weight,
        input_weight,
        decay_param,
        decay_shift,
        mix_output,
        second_gain,
        second_gate,
        second_up,
        second_down,
        final_gain,
    ) = arrays
    rows, width = tokens.shape
    d = width * m
    units = first_gate.shape[1]
    lanes = mix_input.shape[1]
    h, q, chips = n // 2, n // m, m // 2
    split = units % 256 == 0 and h % 4 == 0 and h & (h - 1) == 0
    part_units = units // 2 if split else units
    hbm = pl.BlockSpec(memory_space=pl.ANY)
    vmem = pl.BlockSpec(memory_space=pltpu.VMEM)
    dma = pltpu.SemaphoreType.DMA
    spare = pltpu.VMEM((16, 128), BF16)
    return pl.pallas_call(
        functools.partial(kernel, n, m, split),
        out_shape=jax.ShapeDtypeStruct((rows, width), BF16),
        in_specs=[hbm] * 10 + [vmem] * 9,
        out_specs=vmem,
        scratch_shapes=[
            *[pltpu.VMEM((d, part_units), BF16)] * 3,
            *[pltpu.VMEM((d, lanes), BF16)] * 3,
            *[pltpu.VMEM((d, units), BF16)] * 3,
            pltpu.VMEM((rows, d), BF16),
            pltpu.VMEM((rows, d), BF16) if split else spare,
            pltpu.VMEM((rows, d), BF16),
            pltpu.VMEM((rows, d), BF16) if split else spare,
            pltpu.VMEM((rows, units), BF16),
            pltpu.VMEM((2 * rows, part_units), BF16) if split else spare,
            pltpu.VMEM((rows, chips * width), BF16),
            pltpu.VMEM((rows, chips * width), BF16) if split else spare,
            pltpu.VMEM((rows, max(chips - 1, 1) * width), BF16),
            pltpu.VMEM((rows, max(chips - 1, 1) * width), BF16) if split else spare,
            pltpu.VMEM((rows, width), BF16) if split else spare,
            pltpu.VMEM((rows, lanes), BF16),
            pltpu.VMEM((rows + 8, lanes), F32),
            pltpu.VMEM((rows, lanes), F32),
            pltpu.VMEM((rows, lanes), F32),
            pltpu.VMEM((rows, lanes), F32),
            pltpu.VMEM((lanes, lanes), BF16),
            pltpu.VMEM((lanes, lanes), BF16),
            pltpu.VMEM((8, rows), F32),
            pltpu.VMEM((m - 1, 8, rows), F32),
            dma((10, 2, h)),
            dma((10, 2, h)),
            dma((11,)),
            dma((4, chips)),
            dma((4, chips)),
            dma((4, chips)),
            dma((4, chips)),
            dma((4, 2 * n)),
            dma((4, n)),
            dma((4, 2 * n)),
            dma((4, max(chips - 1, 1) * q * 2)),
            dma((m,)),
            dma((m,)),
            dma((6, h)),
            dma((6, h)),
            dma((6, h)),
            dma((6, h)),
            dma((2,)),
            dma((2,)),
        ],
        compiler_params=pltpu.CompilerParams(
            collective_id=0, has_side_effects=True, vmem_limit_bytes=67043328
        ),
        cost_estimate=pl.CostEstimate(
            flops=rows * d * (12 * units + 6 * lanes), bytes_accessed=8 * d * units, transcendentals=0
        ),
    )(
        tokens,
        first_gate,
        first_up,
        first_down,
        mix_input,
        mix_branch,
        mix_output,
        second_gate,
        second_up,
        second_down,
        first_gain[None, :],
        mix_gain[None, :],
        second_gain[None, :],
        conv_weight,
        rate_weight,
        input_weight,
        decay_param[None, :],
        decay_shift.T,
        final_gain[None, :],
    )


def solution(mesh):
    return jax.shard_map(
        functools.partial(shards, mesh.shape["fs"], mesh.shape["tp"]),
        mesh=mesh,
        in_specs=(
            P("fs", "tp"),
            P(),
            P("fs", "tp"),
            P("fs", "tp"),
            P("fs", "tp"),
            P(),
            P("fs", "tp"),
            P("fs", "tp"),
            P(None, "tp"),
            P("tp", None, None),
            P("tp", None, None),
            P("tp"),
            P("fs", "tp"),
            P("fs", "tp"),
            P(),
            P("fs", "tp"),
            P("fs", "tp"),
            P("fs", "tp"),
            P("tp"),
        ),
        out_specs=P("fs", "tp"),
        check_vma=False,
    )
```

```python
import functools

import jax
import jax.numpy as jnp
from jax import lax
from jax.experimental import pallas as pl
from jax.experimental.pallas import tpu as pltpu
from jax.sharding import PartitionSpec as P

HEAD_DIM = 64
CONV = 4
norm_eps = 1e-06
rate_scale = 8.0
MESH = pl.DeviceIdType.MESH
F32, BF16 = jnp.float32, jnp.bfloat16
G1, U1, D1, MI, MB, MO, G2, U2, D2A, D2B = range(10)


def tile_of(size, *choices):
    for choice in choices:
        if size % choice == 0:
            return choice
    return size


def negative_expm1(y):
    series = 1.0 + y * (1.0 / 6.0)
    for k in (5, 4, 3, 2):
        series = 1.0 + y * (1.0 / k) * series
    return jnp.where(y > -0.25, -y * series, 1.0 - jnp.exp(y))


def scoped(f):
    def g(*args):
        tag = "_".join(str(a) for a in args if isinstance(a, int))
        with jax.named_scope(f"{f.__name__}_{tag}"):
            return f(*args)

    return g


def dot(left, right):
    return jnp.dot(left, right, preferred_element_type=F32)


def dot_last(left, right):
    return lax.dot_general(left, right, (((1,), (1,)), ((), ())), preferred_element_type=F32)


def kernel(
    n,
    m,
    split,
    tokens,
    first_gate,
    first_up,
    first_down,
    mix_input,
    mix_branch,
    mix_output,
    second_gate,
    second_up,
    second_down,
    first_gain,
    mix_gain,
    second_gain,
    conv_weight,
    rate_weight,
    input_weight,
    decay_param,
    decay_shift,
    final_gain,
    out,
    stream,
    w_gate1,
    w_up1,
    w_down1,
    w_in,
    w_branch,
    w_out,
    w_gate2,
    w_up2,
    w_down2,
    gathered,
    gathered_mate,
    normed,
    normed_mate,
    hidden,
    hidden_half,
    near,
    near_mate,
    far,
    far_mate,
    from_mate,
    mixed,
    lane,
    branch,
    decay,
    drive,
    rate_map,
    input_map,
    square_own,
    square_in,
    ring_send,
    ring_recv,
    own_sem,
    ag_near_send,
    ag_near_recv,
    ag_far_send,
    ag_far_recv,
    rs_near_send,
    rs_near_recv,
    rs_far_send,
    rs_far_recv,
    sq_send,
    sq_recv,
    spread_send,
    spread_recv,
    cross_send,
    cross_recv,
    mate_send,
    mate_recv,
):
    h = n // 2
    chips = m // 2
    q = n // m
    rows, width = stream.shape
    d = width * m
    block = d // n
    units = first_gate.shape[1]
    lanes = mix_input.shape[1]
    fs = lax.axis_index("fs")
    tp = lax.axis_index("tp")
    chip = tp // 2
    core = tp % 2
    partner = tp + 1 - 2 * core
    at = jnp.where(fs % 2 == 0, fs // 2, n - 1 - fs // 2)

    def owner(place):
        p = lax.rem(place + 2 * n, n)
        return jnp.where(p < h, 2 * p, 2 * (n - 1 - p) + 1)

    right, left = owner(at + 1), owner(at - 1)
    part_units = w_gate1.shape[1]
    places = n // 2
    line, side = fs // 2, fs % 2

    def flip(value, bits):
        bit = 1
        while bit <= bits:
            if bits & bit:
                value = value + bit - 2 * bit * (value // bit % 2)
            bit *= 2
        return value

    def share(place):
        return (place % 4 + 1) // 2 % 2

    mate = flip(line, 1) * 2 + side
    half = block // 2
    plan = [
        (first_gate, w_gate1, 0, block),
        (first_up, w_up1, 0, block),
        (first_down, w_down1, 0, block),
        (mix_input, w_in, 0, block),
        (mix_branch, w_branch, 0, block),
        (mix_output, w_out, 0, block),
        (second_gate, w_gate2, 0, block),
        (second_up, w_up2, 0, block),
        (second_down, w_down2, 0, half),
        (second_down, w_down2, half, half),
    ]

    ring_low = G2 if split else 0

    def ring_copy(k, way, step, arriving=False):
        source, buffer, low, count = plan[k]
        sign = -1 if way == 0 else 1
        b = owner(at + sign * (step + 1 if arriving else step))
        if step == h - 1:
            count = count // 2
            low = low + way * count
        place = pl.ds(pl.multiple_of(b * block + low, 16), count)
        if step == 0 and not arriving:
            src = source if count == block else source.at[pl.ds(low, count)]
        else:
            src = buffer.at[place]
        return pltpu.make_async_remote_copy(
            src_ref=src,
            dst_ref=buffer.at[place],
            send_sem=ring_send.at[k - ring_low, way, step],
            recv_sem=ring_recv.at[k - ring_low, way, step],
            device_id={"fs": right if way == 0 else left},
            device_id_type=MESH,
        )

    @scoped
    def launch(*ks):
        for k in ks:
            for way in (0, 1):
                ring_copy(k, way, 0).start()

    @scoped
    def serve(k, step):
        for way in (0, 1):
            ring_copy(k, way, step - 1, arriving=True).wait_recv()
            if step < h:
                ring_copy(k, way, step).start()

    barrier = pltpu.get_barrier_semaphore()
    for hop in range(1, n):
        pl.semaphore_signal(
            barrier, inc=1, device_id={"fs": lax.rem(fs + hop, n)}, device_id_type=MESH
        )
    for hop in range(1, m):
        pl.semaphore_signal(
            barrier, inc=1, device_id={"tp": lax.rem(tp + hop, m)}, device_id_type=MESH
        )
    pl.semaphore_wait(barrier, n - 1 + m - 1)

    def columns(index, size):
        return pl.ds(pl.multiple_of(index * size, 128), size)

    def full_of(phase):
        return gathered_mate if phase == 3 else gathered

    def terms_ref(phase):
        return normed_mate if phase == 3 else normed

    def near_of(phase):
        return near_mate if phase == 3 else near

    def far_of(phase):
        return far_mate if phase == 3 else far

    def gather_far(phase, hop, source):
        return pltpu.make_async_remote_copy(
            src_ref=source,
            dst_ref=full_of(phase).at[:, columns(tp, width)],
            send_sem=ag_far_send.at[phase, hop],
            recv_sem=ag_far_recv.at[phase, hop],
            device_id={"tp": lax.rem(tp + 2 * hop, m)},
            device_id_type=MESH,
        )

    def gather_near(phase, hop, source=None, arriving=False):
        origin = lax.rem((partner if arriving else tp) - 2 * hop + 2 * m, m)
        place = full_of(phase).at[:, columns(origin, width)]
        return pltpu.make_async_remote_copy(
            src_ref=place if source is None else source,
            dst_ref=place,
            send_sem=ag_near_send.at[phase, hop],
            recv_sem=ag_near_recv.at[phase, hop],
            device_id={"tp": partner},
            device_id_type=MESH,
        )

    def gather_arrived_far(phase, hop):
        origin = lax.rem(tp - 2 * hop + 2 * m, m)
        place = full_of(phase).at[:, columns(origin, width)]
        return pltpu.make_async_remote_copy(
            src_ref=place,
            dst_ref=place,
            send_sem=ag_far_send.at[phase, hop],
            recv_sem=ag_far_recv.at[phase, hop],
            device_id={"tp": origin},
            device_id_type=MESH,
        )

    @scoped
    def gather_start(phase, source):
        for hop in range(1, chips):
            gather_far(phase, hop, source).start()
        gather_near(phase, 0, source).start()

    @scoped
    def gather_forward(phase):
        for hop in range(1, chips):
            gather_arrived_far(phase, hop).wait_recv()
            gather_near(phase, hop).start()

    @scoped
    def gather_finish(phase, source):
        for hop in range(chips):
            gather_near(phase, hop, arriving=True).wait_recv()
            gather_near(phase, hop, source if hop == 0 else None).wait_send()
        for hop in range(1, chips):
            gather_far(phase, hop, source).wait_send()

    @scoped
    def normalise(gain, phase=0):
        size = tile_of(rows, 64)

        @pl.loop(0, rows // size)
        def _(i):
            place = pl.ds(pl.multiple_of(i * size, size), size)
            values = full_of(phase)[place, :].astype(F32)
            scale = lax.rsqrt(jnp.mean(values * values, axis=-1, keepdims=True) + norm_eps)
            terms_ref(phase)[place, :] = (values * scale * gain[...]).astype(BF16)

    row_tile = tile_of(rows, 256)

    def hidden_view(size):
        return hidden if size == hidden.shape[1] else hidden_half

    @scoped
    def hidden_part(gate, up, part, parts, phase=2):
        size = gate.shape[1]
        unit_tile = tile_of(size, 256, 640, 128)
        across = size // unit_tile
        count = rows // row_tile * across // parts
        first = rows if phase == 3 else 0
        source = terms_ref(phase)
        goal = hidden_view(size)

        @pl.loop(part * count, (part + 1) * count)
        def _(i):
            start = pl.multiple_of((i // across) * row_tile, row_tile)
            place = pl.ds(start, row_tile)
            cols = columns(i % across, unit_tile)
            gate_value = dot(source[place, :], gate[:, cols])
            up_value = dot(source[place, :], up[:, cols])
            goal[pl.ds(start + first, row_tile), cols] = (
                jax.nn.silu(gate_value) * up_value
            ).astype(BF16)

    def grain(phase):
        return half if phase == 2 and half % 128 == 0 else block

    def pieces(phase):
        return width // grain(phase)

    def near_copy(phase, b):
        q, block = pieces(phase), grain(phase)
        slot = b // q // 2 * q + b % q
        return pltpu.make_async_remote_copy(
            src_ref=terms_ref(phase).at[:, columns(b, block)],
            dst_ref=near_of(phase).at[:, columns(slot, block)],
            send_sem=rs_near_send.at[phase // 3, b],
            recv_sem=rs_near_recv.at[phase, slot],
            device_id={"tp": partner},
            device_id_type=MESH,
        )

    def far_copy(phase, b):
        q, block = pieces(phase), grain(phase)
        to_chip = b // q // 2
        hop = lax.rem(to_chip - chip + chips, chips)
        slot = (hop - 1) * q + b % q
        return pltpu.make_async_remote_copy(
            src_ref=terms_ref(phase).at[:, columns(b, block)],
            dst_ref=far_of(phase).at[:, columns(slot, block)],
            send_sem=rs_far_send.at[phase // 3, b],
            recv_sem=rs_far_recv.at[phase, slot],
            device_id={"tp": to_chip * 2 + core},
            device_id_type=MESH,
        )

    @scoped
    def terms_of(phase, left_ref, weight, b):
        q, block = pieces(phase), grain(phase)
        first = rows if phase == 3 else 0
        tall = tile_of(rows, 512)
        weights = pl.ds(pl.multiple_of(b * block, block), block)

        @pl.loop(0, rows // tall)
        def _(i):
            place = pl.ds(pl.multiple_of(i * tall, tall), tall)
            inner = pl.ds(pl.multiple_of(i * tall + first, tall), tall)
            value = dot_last(left_ref[inner, :], weight[weights, :])
            terms_ref(phase)[place, columns(b, block)] = value.astype(BF16)

        @pl.when(b // q % 2 != core)
        def _():
            near_copy(phase, b).start()

    @scoped
    def pass_on(phase, b):
        q, block = pieces(phase), grain(phase)
        mine = b // q % 2 == core
        slot = b // q // 2 * q + b % q

        @pl.when(mine)
        def _():
            near_copy(phase, b).wait_recv()

        @pl.when(mine & (b // q // 2 != chip))
        def _():
            @pl.loop(0, rows // row_tile)
            def _(i):
                place = pl.ds(pl.multiple_of(i * row_tile, row_tile), row_tile)
                total = terms_ref(phase)[place, columns(b, block)].astype(F32)
                total = total + near_of(phase)[place, columns(slot, block)].astype(F32)
                terms_ref(phase)[place, columns(b, block)] = total.astype(BF16)

            far_copy(phase, b).start()

    def turn(b):
        return lax.rem(b + (chip + 1) * (n // chips), n)

    def blocks_at(step):
        if step == 0:
            return [fs]
        if step == h:
            return [owner(at + h)]
        return [owner(at - step), owner(at + step)]

    def far_arrived(phase, hop, k):
        q, block = pieces(phase), grain(phase)
        slot = (hop - 1) * q + k
        place = far_of(phase).at[:, slot * block : (slot + 1) * block]
        return pltpu.make_async_remote_copy(
            src_ref=place,
            dst_ref=place,
            send_sem=rs_far_send.at[phase // 3, 0],
            recv_sem=rs_far_recv.at[phase, slot],
            device_id={"tp": partner},
            device_id_type=MESH,
        )

    def sum_of(phase, place):
        total = terms_ref(phase)[place, columns(tp, width)].astype(F32)
        total = total + near_of(phase)[place, columns(chip, width)].astype(F32)
        for hop in range(1, chips):
            total = total + far_of(phase)[place, (hop - 1) * width : hop * width].astype(F32)
        return total

    chunks = 1
    chunk = rows // chunks

    def mate_copy(which, c):
        cols = columns(tp, width)
        part = pl.ds(c * chunk, chunk)
        return pltpu.make_async_remote_copy(
            src_ref=normed_mate.at[part, cols] if which else tokens.at[part],
            dst_ref=from_mate.at[part] if which else gathered_mate.at[part, cols],
            send_sem=mate_send.at[which, c],
            recv_sem=mate_recv.at[which, c],
            device_id={"fs": mate},
            device_id_type=MESH,
        )

    def mate_start(which):
        for c in range(chunks):
            mate_copy(which, c).start()

    def mate_arrived(which):
        for c in range(chunks):
            mate_copy(which, c).wait_recv()

    @scoped
    def finish_mate():
        for hop in range(1, chips):
            for k in range(pieces(3)):
                far_arrived(3, hop, k).wait_recv()

        @pl.loop(0, rows // row_tile)
        def _(i):
            place = pl.ds(pl.multiple_of(i * row_tile, row_tile), row_tile)
            normed_mate[place, columns(tp, width)] = sum_of(3, place).astype(BF16)

        mate_start(1)

    @scoped
    def finish_sum(phase, factor, whole):
        for hop in range(1, chips):
            for k in range(pieces(phase)):
                far_arrived(phase, hop, k).wait_recv()
        if phase == 0 and split:
            mate_arrived(1)
            launch(U2)

        @pl.loop(0, rows // row_tile)
        def _(i):
            place = pl.ds(pl.multiple_of(i * row_tile, row_tile), row_tile)
            total = sum_of(phase, place)
            if phase == 0 and split:
                total = total + from_mate[place, :].astype(F32)
            value = (stream[place, :].astype(F32) + factor * total).astype(BF16)
            stream[place, :] = value
            if whole:
                gathered[place, columns(tp, width)] = value

    @scoped
    def sent_sum(phase):
        q = pieces(phase)
        for b in range(q * m):

            @pl.when(b // q % 2 != core)
            def _():
                near_copy(phase, b).wait_send()

            @pl.when((b // q % 2 == core) & (b // q // 2 != chip))
            def _():
                far_copy(phase, b).wait_send()

    def piece_of(k):
        if k < 6:
            return (*plan[k // 2][:2], k % 2 * half, half)
        return plan[k - 3]

    def part_rows(k, place, beside):
        low, count = piece_of(k)[2:]
        return pl.ds(pl.multiple_of((place * 2 + beside) * block + low, 16), count)

    def own_part(k, place):
        source, _, low, count = piece_of(k)
        if k >= 6:
            return source
        return source.at[low : low + count, columns(share(place), part_units)]

    def spread_copy(k, bits):
        other = flip(line, bits)
        return pltpu.make_async_remote_copy(
            src_ref=own_part(k, other),
            dst_ref=piece_of(k)[1].at[part_rows(k, line, side)],
            send_sem=spread_send.at[k % 3, bits],
            recv_sem=spread_recv.at[k, bits],
            device_id={"fs": other * 2 + side},
            device_id_type=MESH,
        )

    def spread_arrived(k, bits):
        place = piece_of(k)[1].at[part_rows(k, flip(line, bits), side)]
        return pltpu.make_async_remote_copy(
            src_ref=place,
            dst_ref=place,
            send_sem=spread_send.at[k % 3, bits],
            recv_sem=spread_recv.at[k, bits],
            device_id={"fs": mate},
            device_id_type=MESH,
        )

    def cross_copy(k, bits, arriving=False):
        beside = 1 - side if arriving else side
        place = piece_of(k)[1].at[part_rows(k, flip(line, bits), beside)]
        return pltpu.make_async_remote_copy(
            src_ref=own_part(k, line) if bits == 0 and not arriving else place,
            dst_ref=place,
            send_sem=cross_send.at[k, bits],
            recv_sem=cross_recv.at[k, bits],
            device_id={"fs": fs + 1 - 2 * side},
            device_id_type=MESH,
        )

    mixes = range(6, 9)
    last_first = [*range(2, places), 1]

    @scoped
    def cross(k):
        for bits in last_first:
            spread_arrived(k, bits).wait_recv()
            cross_copy(k, bits).start()
            spread_copy(k, bits).wait_send()
            if k + 2 < 6:
                spread_copy(k + 2, bits).start()

    @scoped
    def crossed(*parts):
        for part in parts:
            for bits in range(places):
                cross_copy(part, bits, arriving=True).wait_recv()

    if split:
        for bits in range(1, places):
            spread_copy(0, bits).start()
        for k in range(6):
            cross_copy(k, 0).start()
    else:
        launch(G1, U1)
    gather_start(0, tokens)
    own = [
        pltpu.make_async_copy(tokens, stream, own_sem.at[0]),
        pltpu.make_async_copy(tokens, gathered.at[:, columns(tp, width)], own_sem.at[1]),
    ]
    mine = pl.ds(pl.multiple_of(fs * block, block), block)
    for k in range(9):
        source, buffer, _, _ = plan[k]
        if split and k in (G1, U1, D1):
            source = source.at[:, columns(share(line), part_units)]
        own.append(pltpu.make_async_copy(source, buffer.at[mine], own_sem.at[2 + k]))
    for copy in own:
        copy.start()
    rate_map[...] = jnp.zeros_like(rate_map)
    input_map[...] = jnp.zeros_like(input_map)
    for k in range(lanes // HEAD_DIM):
        part = slice(k * HEAD_DIM, (k + 1) * HEAD_DIM)
        rate_map[part, part] = rate_weight[k]
        input_map[part, part] = input_weight[k]
    lane[0:8, :] = jnp.zeros((8, lanes), F32)
    with jax.named_scope("ownwait"):
        for copy in own:
            copy.wait()

    if split:
        own_cols = gathered_mate.at[:, columns(tp, width)]
        for bits in range(1, places):
            spread_copy(1, bits).start()
        cross(0)
        mate_start(0)
        gather_forward(0)
        cross(1)
        gather_finish(0, tokens)
        normalise(first_gain)
        cross(2)
        with jax.named_scope("matewait"):
            mate_arrived(0)
        gather_start(3, own_cols)
        cross(3)
        cross(4)
        gather_forward(3)
        cross(5)
        for k in mixes:
            for bits in range(1, places):
                spread_copy(k, bits).start()
        gather_finish(3, own_cols)
        normalise(first_gain, 3)
        crossed(0, 1, 2, 3)
        hidden_part(w_gate1, w_up1, 0, 1, 3)
        crossed(4, 5)
        launch(G2)
        for k in mixes:
            cross_copy(k, 0).start()
        for b in range(n):
            terms_of(3, hidden_half, w_down1, turn(b))
            if b:
                pass_on(3, turn(b - 1))
        pass_on(3, turn(n - 1))
        hidden_part(w_gate1, w_up1, 0, 1, 0)
        for b in range(n):
            terms_of(0, hidden_half, w_down1, turn(b))
            if b:
                pass_on(0, turn(b - 1))
            if b == n // 2 - 1:
                finish_mate()
        pass_on(0, turn(n - 1))
        for k in mixes:
            cross(k)
    else:
        serve(G1, 1)
        gather_forward(0)
        serve(U1, 1)
        gather_finish(0, tokens)
        normalise(first_gain)
        for step in range(2, h + 1):
            serve(G1, step)
            serve(U1, step)
            if step == h - 1:
                launch(D1)
        launch(MI, MB, MO)
        hidden_part(w_gate1, w_up1, 0, 1, 0)
        for b in blocks_at(0):
            terms_of(0, hidden, w_down1, b)
        for step in range(1, h + 1):
            serve(D1, step)
            for b in blocks_at(step):
                terms_of(0, hidden, w_down1, b)
            for k in (MI, MB, MO):
                serve(k, step)
            for b in blocks_at(step - 1):
                pass_on(0, b)
            if step == h - 1:
                launch(G2, U2)
        for b in blocks_at(h):
            pass_on(0, b)
    finish_sum(0, 0.5, True)
    gather_start(1, stream)
    sent_sum(0)
    if split:
        sent_sum(3)

    queue = [(k, step) for step in range(1, h + 1) for k in (G2, U2)]

    def take(count):
        for _ in range(min(count, len(queue))):
            k, step = queue.pop(0)
            serve(k, step)
            if (k, step) == (G2, h):
                launch(D2A)
            if (k, step) == (U2, h):
                launch(D2B)

    take(1)
    gather_forward(1)
    take(1)
    gather_finish(1, stream)
    normalise(mix_gain)
    if split:
        crossed(*mixes)

    @pl.loop(0, rows // row_tile)
    def _(i):
        place = pl.ds(pl.multiple_of(i * row_tile, row_tile), row_tile)
        lower = pl.ds(pl.multiple_of(i * row_tile + 8, 8), row_tile)
        value = dot(normed[place, :], w_in[...])
        lane[lower, :] = value.astype(BF16).astype(F32)
        branch[place, :] = dot(normed[place, :], w_branch[...])

    take(1)
    slope = -rate_scale * jnp.log1p(jnp.exp(-decay_param[...]))
    small = tile_of(rows, 128)

    @pl.loop(0, rows // small)
    def _(i):
        place = pl.ds(pl.multiple_of(i * small, small), small)
        upper = lane[pl.ds(pl.multiple_of(i * small, 8), small + 8), :]
        conv_sum = jnp.zeros((small, lanes), F32)
        for k in range(CONV):
            shifted = pltpu.roll(upper, CONV - 1 - k, 0) if k < CONV - 1 else upper
            conv_sum = conv_sum + shifted[8:, :] * conv_weight[k : k + 1, :].astype(F32)
        conv_out = conv_sum.astype(BF16)
        rate = jax.nn.sigmoid(dot(conv_out, rate_map[...]))
        admit = jax.nn.sigmoid(dot(conv_out, input_map[...]))
        shifts = decay_shift[:, columns(i, small)]
        shift = jnp.concatenate(
            [
                jnp.broadcast_to(shifts[k : k + 1, :], (HEAD_DIM, small))
                for k in range(lanes // HEAD_DIM)
            ],
            axis=0,
        ).T
        log_decay = rate * slope + shift
        decay[place, :] = jnp.exp(log_decay)
        drive[place, :] = (
            jnp.sqrt(negative_expm1(2.0 * log_decay)) * admit * conv_out.astype(F32)
        )

    lane_tile = tile_of(lanes, 128)
    row_id = lax.broadcasted_iota(jnp.int32, (rows, lane_tile), 0)

    @pl.loop(0, lanes // lane_tile)
    def _(i):
        cols = columns(i, lane_tile)
        factor, state = decay[:, cols], drive[:, cols]
        reach = 1
        while reach < rows:
            inside = row_id >= reach
            state = factor * jnp.where(inside, pltpu.roll(state, reach, 0), 0.0) + state
            if reach * 2 < rows:
                factor = factor * jnp.where(inside, pltpu.roll(factor, reach, 0), 1.0)
            reach *= 2
        mixed[:, cols] = (state * jax.nn.gelu(branch[:, cols])).astype(BF16)

    for b in range(n):
        terms_of(1, mixed, w_out, turn(b))
        if b:
            pass_on(1, turn(b - 1))
    pass_on(1, turn(n - 1))
    take(2)
    finish_sum(1, 1.0, True)
    gather_start(2, stream)
    sent_sum(1)
    take(2 * h)
    gather_forward(2)
    halves = [(k, step) for step in range(1, h + 1) for k in (D2A, D2B)]
    serve(*halves.pop(0))
    gather_finish(2, stream)
    normalise(second_gain)

    parts = tile_of(rows // row_tile, 4, 2)
    for part in range(parts):
        hidden_part(w_gate2, w_up2, part, parts)
        if part < 2:
            serve(*halves.pop(0))
    fine = block // grain(2)
    for step in range(h + 1):
        for piece in range(2):
            reach = (step, D2A + piece)
            if step == 0:
                reach = (2 * piece, D2B)
            elif (step, piece) == (1, 1):
                reach = (3, D2A)
            while halves and (halves[0][1], halves[0][0]) <= reach:
                serve(*halves.pop(0))
            if fine == 1 and piece == 0:
                continue
            fresh = [
                b * fine + e for b in blocks_at(step) for e in ([piece] if fine == 2 else [0])
            ]
            for b in fresh:
                terms_of(2, hidden, w_down2, b)
            for b in fresh:
                pass_on(2, b)
    finish_sum(2, 0.5, False)

    @pl.loop(0, rows // row_tile)
    def _(i):
        place = pl.ds(pl.multiple_of(i * row_tile, row_tile), row_tile)
        values = stream[place, :].astype(F32)
        squares = jnp.sum(values * values, axis=-1, keepdims=True)
        square_own[:, columns(i, row_tile)] = jnp.broadcast_to(squares, (row_tile, 128)).T[:8, :]

    def square_copy(hop):
        return pltpu.make_async_remote_copy(
            src_ref=square_own,
            dst_ref=square_in.at[hop - 1],
            send_sem=sq_send.at[hop],
            recv_sem=sq_recv.at[hop],
            device_id={"tp": lax.rem(tp + hop, m)},
            device_id_type=MESH,
        )

    for hop in range(1, m):
        square_copy(hop).start()
    sent_sum(2)
    for k in range(G2 if split else 0, len(plan)):
        for way in (0, 1):
            for step in range(h):
                ring_copy(k, way, step).wait_send()
    if split:
        for k in range(9):
            for bits in range(places):
                cross_copy(k, bits).wait_send()
        for which in range(2):
            for c in range(chunks):
                mate_copy(which, c).wait_send()
    with jax.named_scope("sqwait"):
        for hop in range(1, m):
            square_copy(hop).wait()

    def out_copy(i):
        place = pl.ds(i * row_tile, row_tile)
        return pltpu.make_async_copy(stream.at[place], out.at[place], own_sem.at[i])

    with jax.named_scope("final"):
        for i in range(rows // row_tile):
            place = slice(i * row_tile, (i + 1) * row_tile)
            squares = square_own[:, place]
            for hop in range(1, m):
                squares = squares + square_in[hop - 1, :, place]
            spread = jnp.broadcast_to(squares[0:1, :], (128, row_tile)).T
            scale = lax.rsqrt(spread[:, 0:1] / d + norm_eps)
            stream[place, :] = (stream[place, :].astype(F32) * scale * final_gain[...]).astype(BF16)
            out_copy(i).start()
    with jax.named_scope("outwait"):
        for i in range(rows // row_tile):
            out_copy(i).wait()


def shards(n, m, *arrays):
    (
        tokens,
        first_gain,
        first_gate,
        first_up,
        first_down,
        mix_gain,
        mix_input,
        mix_branch,
        conv_weight,
        rate_weight,
        input_weight,
        decay_param,
        decay_shift,
        mix_output,
        second_gain,
        second_gate,
        second_up,
        second_down,
        final_gain,
    ) = arrays
    rows, width = tokens.shape
    d = width * m
    units = first_gate.shape[1]
    lanes = mix_input.shape[1]
    h, q, chips = n // 2, n // m, m // 2
    split = units % 256 == 0 and h % 4 == 0 and h & (h - 1) == 0
    part_units = units // 2 if split else units
    hbm = pl.BlockSpec(memory_space=pl.ANY)
    vmem = pl.BlockSpec(memory_space=pltpu.VMEM)
    dma = pltpu.SemaphoreType.DMA
    spare = pltpu.VMEM((16, 128), BF16)
    return pl.pallas_call(
        functools.partial(kernel, n, m, split),
        out_shape=jax.ShapeDtypeStruct((rows, width), BF16),
        in_specs=[hbm] * 10 + [vmem] * 9,
        out_specs=hbm,
        scratch_shapes=[
            pltpu.VMEM((rows, width), BF16),
            *[pltpu.VMEM((d, part_units), BF16)] * 3,
            *[pltpu.VMEM((d, lanes), BF16)] * 3,
            *[pltpu.VMEM((d, units), BF16)] * 3,
            pltpu.VMEM((rows, d), BF16),
            pltpu.VMEM((rows, d), BF16) if split else spare,
            pltpu.VMEM((rows, d), BF16),
            pltpu.VMEM((rows, d), BF16) if split else spare,
            pltpu.VMEM((rows, units), BF16),
            pltpu.VMEM((2 * rows, part_units), BF16) if split else spare,
            pltpu.VMEM((rows, chips * width), BF16),
            pltpu.VMEM((rows, chips * width), BF16) if split else spare,
            pltpu.VMEM((rows, max(chips - 1, 1) * width), BF16),
            pltpu.VMEM((rows, max(chips - 1, 1) * width), BF16) if split else spare,
            pltpu.VMEM((rows, width), BF16) if split else spare,
            pltpu.VMEM((rows, lanes), BF16),
            pltpu.VMEM((rows + 8, lanes), F32),
            pltpu.VMEM((rows, lanes), F32),
            pltpu.VMEM((rows, lanes), F32),
            pltpu.VMEM((rows, lanes), F32),
            pltpu.VMEM((lanes, lanes), BF16),
            pltpu.VMEM((lanes, lanes), BF16),
            pltpu.VMEM((8, rows), F32),
            pltpu.VMEM((m - 1, 8, rows), F32),
            dma((4 if split else 10, 2, h)),
            dma((4 if split else 10, 2, h)),
            dma((11,)),
            dma((4, chips)),
            dma((4, chips)),
            dma((4, chips)),
            dma((4, chips)),
            dma((2, 2 * n)),
            dma((4, n)),
            dma((2, 2 * n)),
            dma((4, max(chips - 1, 1) * q * 2)),
            dma((m,)),
            dma((m,)),
            dma((3, h)),
            dma((9, h)),
            dma((9, h)),
            dma((9, h)),
            dma((2, 1)),
            dma((2, 1)),
        ],
        compiler_params=pltpu.CompilerParams(
            collective_id=0, has_side_effects=True, vmem_limit_bytes=67043328
        ),
        cost_estimate=pl.CostEstimate(
            flops=rows * d * (12 * units + 6 * lanes), bytes_accessed=8 * d * units, transcendentals=0
        ),
    )(
        tokens,
        first_gate,
        first_up,
        first_down,
        mix_input,
        mix_branch,
        mix_output,
        second_gate,
        second_up,
        second_down,
        first_gain[None, :],
        mix_gain[None, :],
        second_gain[None, :],
        conv_weight,
        rate_weight,
        input_weight,
        decay_param[None, :],
        decay_shift.T,
        final_gain[None, :],
    )


def solution(mesh):
    return jax.shard_map(
        functools.partial(shards, mesh.shape["fs"], mesh.shape["tp"]),
        mesh=mesh,
        in_specs=(
            P("fs", "tp"),
            P(),
            P("fs", "tp"),
            P("fs", "tp"),
            P("fs", "tp"),
            P(),
            P("fs", "tp"),
            P("fs", "tp"),
            P(None, "tp"),
            P("tp", None, None),
            P("tp", None, None),
            P("tp"),
            P("fs", "tp"),
            P("fs", "tp"),
            P(),
            P("fs", "tp"),
            P("fs", "tp"),
            P("fs", "tp"),
            P("tp"),
        ),
        out_specs=P("fs", "tp"),
        check_vma=False,
    )
```

```python
import functools

import jax
import jax.numpy as jnp
from jax import lax
from jax.experimental import pallas as pl
from jax.experimental.pallas import tpu as pltpu
from jax.sharding import PartitionSpec as P

HEAD_DIM = 64
CONV = 4
norm_eps = 1e-06
rate_scale = 8.0
MESH = pl.DeviceIdType.MESH
F32, BF16 = jnp.float32, jnp.bfloat16
G1, U1, D1, MI, MB, MO, G2, U2, D2A, D2B = range(10)


def tile_of(size, *choices):
    for choice in choices:
        if size % choice == 0:
            return choice
    return size


def negative_expm1(y):
    series = 1.0 + y * (1.0 / 6.0)
    for k in (5, 4, 3, 2):
        series = 1.0 + y * (1.0 / k) * series
    return jnp.where(y > -0.25, -y * series, 1.0 - jnp.exp(y))


def scoped(f):
    def g(*args):
        tag = "_".join(str(a) for a in args if isinstance(a, int))
        with jax.named_scope(f"{f.__name__}_{tag}"):
            return f(*args)

    return g


def dot(left, right):
    return jnp.dot(left, right, preferred_element_type=F32)


def dot_last(left, right):
    return lax.dot_general(left, right, (((1,), (1,)), ((), ())), preferred_element_type=F32)


def kernel(
    n,
    m,
    split,
    tokens,
    first_gate,
    first_up,
    first_down,
    mix_input,
    mix_branch,
    mix_output,
    second_gate,
    second_up,
    second_down,
    first_gain,
    mix_gain,
    second_gain,
    conv_weight,
    rate_weight,
    input_weight,
    decay_param,
    decay_shift,
    final_gain,
    out,
    stream,
    w_gate1,
    w_up1,
    w_down1,
    w_in,
    w_branch,
    w_out,
    w_gate2,
    w_up2,
    w_down2,
    gathered,
    gathered_mate,
    normed,
    normed_mate,
    hidden,
    hidden_half,
    near,
    near_mate,
    far,
    far_mate,
    from_mate,
    mixed,
    lane,
    branch,
    decay,
    drive,
    rate_map,
    input_map,
    square_own,
    square_in,
    ring_send,
    ring_recv,
    own_sem,
    ag_near_send,
    ag_near_recv,
    ag_far_send,
    ag_far_recv,
    rs_near_send,
    rs_near_recv,
    rs_far_send,
    rs_far_recv,
    sq_send,
    sq_recv,
    spread_send,
    spread_recv,
    cross_send,
    cross_recv,
    mate_send,
    mate_recv,
):
    h = n // 2
    chips = m // 2
    q = n // m
    rows, width = stream.shape
    d = width * m
    block = d // n
    units = first_gate.shape[1]
    lanes = mix_input.shape[1]
    fs = lax.axis_index("fs")
    tp = lax.axis_index("tp")
    chip = tp // 2
    core = tp % 2
    partner = tp + 1 - 2 * core
    at = jnp.where(fs % 2 == 0, fs // 2, n - 1 - fs // 2)

    def owner(place):
        p = lax.rem(place + 2 * n, n)
        return jnp.where(p < h, 2 * p, 2 * (n - 1 - p) + 1)

    right, left = owner(at + 1), owner(at - 1)
    part_units = w_gate1.shape[1]
    places = n // 2
    line, side = fs // 2, fs % 2

    def flip(value, bits):
        bit = 1
        while bit <= bits:
            if bits & bit:
                value = value + bit - 2 * bit * (value // bit % 2)
            bit *= 2
        return value

    def share(place):
        return (place % 4 + 1) // 2 % 2

    mate = flip(line, 1) * 2 + side
    half = block // 2
    plan = [
        (first_gate, w_gate1, 0, block),
        (first_up, w_up1, 0, block),
        (first_down, w_down1, 0, block),
        (mix_input, w_in, 0, block),
        (mix_branch, w_branch, 0, block),
        (mix_output, w_out, 0, block),
        (second_gate, w_gate2, 0, block),
        (second_up, w_up2, 0, block),
        (second_down, w_down2, 0, half),
        (second_down, w_down2, half, half),
    ]

    ring_low = G2 if split else 0

    def ring_copy(k, way, step, arriving=False):
        source, buffer, low, count = plan[k]
        sign = -1 if way == 0 else 1
        b = owner(at + sign * (step + 1 if arriving else step))
        if step == h - 1:
            count = count // 2
            low = low + way * count
        place = pl.ds(pl.multiple_of(b * block + low, 16), count)
        if step == 0 and not arriving:
            src = source if count == block else source.at[pl.ds(low, count)]
        else:
            src = buffer.at[place]
        return pltpu.make_async_remote_copy(
            src_ref=src,
            dst_ref=buffer.at[place],
            send_sem=ring_send.at[k - ring_low, way, step],
            recv_sem=ring_recv.at[k - ring_low, way, step],
            device_id={"fs": right if way == 0 else left},
            device_id_type=MESH,
        )

    @scoped
    def launch(*ks):
        for k in ks:
            for way in (0, 1):
                ring_copy(k, way, 0).start()

    @scoped
    def serve(k, step):
        for way in (0, 1):
            ring_copy(k, way, step - 1, arriving=True).wait_recv()
            if step < h:
                ring_copy(k, way, step).start()

    barrier = pltpu.get_barrier_semaphore()
    for hop in range(1, n):
        pl.semaphore_signal(
            barrier, inc=1, device_id={"fs": lax.rem(fs + hop, n)}, device_id_type=MESH
        )
    for hop in range(1, m):
        pl.semaphore_signal(
            barrier, inc=1, device_id={"tp": lax.rem(tp + hop, m)}, device_id_type=MESH
        )
    pl.semaphore_wait(barrier, n - 1 + m - 1)

    def columns(index, size):
        return pl.ds(pl.multiple_of(index * size, 128), size)

    def full_of(phase):
        return gathered_mate if phase == 3 else gathered

    def terms_ref(phase):
        return normed_mate if phase == 3 else normed

    def near_of(phase):
        return near_mate if phase == 3 else near

    def far_of(phase):
        return far_mate if phase == 3 else far

    def gather_far(phase, hop, source):
        return pltpu.make_async_remote_copy(
            src_ref=source,
            dst_ref=full_of(phase).at[:, columns(tp, width)],
            send_sem=ag_far_send.at[phase, hop],
            recv_sem=ag_far_recv.at[phase, hop],
            device_id={"tp": lax.rem(tp + 2 * hop, m)},
            device_id_type=MESH,
        )

    def gather_near(phase, hop, source=None, arriving=False):
        origin = lax.rem((partner if arriving else tp) - 2 * hop + 2 * m, m)
        place = full_of(phase).at[:, columns(origin, width)]
        return pltpu.make_async_remote_copy(
            src_ref=place if source is None else source,
            dst_ref=place,
            send_sem=ag_near_send.at[phase, hop],
            recv_sem=ag_near_recv.at[phase, hop],
            device_id={"tp": partner},
            device_id_type=MESH,
        )

    def gather_arrived_far(phase, hop):
        origin = lax.rem(tp - 2 * hop + 2 * m, m)
        place = full_of(phase).at[:, columns(origin, width)]
        return pltpu.make_async_remote_copy(
            src_ref=place,
            dst_ref=place,
            send_sem=ag_far_send.at[phase, hop],
            recv_sem=ag_far_recv.at[phase, hop],
            device_id={"tp": origin},
            device_id_type=MESH,
        )

    @scoped
    def gather_start(phase, source):
        for hop in range(1, chips):
            gather_far(phase, hop, source).start()
        gather_near(phase, 0, source).start()

    @scoped
    def gather_forward(phase):
        for hop in range(1, chips):
            gather_arrived_far(phase, hop).wait_recv()
            gather_near(phase, hop).start()

    @scoped
    def gather_finish(phase, source):
        for hop in range(chips):
            gather_near(phase, hop, arriving=True).wait_recv()
            gather_near(phase, hop, source if hop == 0 else None).wait_send()
        for hop in range(1, chips):
            gather_far(phase, hop, source).wait_send()

    @scoped
    def normalise(gain, phase=0):
        size = tile_of(rows, 64)

        @pl.loop(0, rows // size)
        def _(i):
            place = pl.ds(pl.multiple_of(i * size, size), size)
            values = full_of(phase)[place, :].astype(F32)
            scale = lax.rsqrt(jnp.mean(values * values, axis=-1, keepdims=True) + norm_eps)
            terms_ref(phase)[place, :] = (values * scale * gain[...]).astype(BF16)

    row_tile = tile_of(rows, 256)

    def hidden_view(size):
        return hidden if size == hidden.shape[1] else hidden_half

    @scoped
    def hidden_part(gate, up, part, parts, phase=2):
        size = gate.shape[1]
        unit_tile = tile_of(size, 256, 640, 128)
        across = size // unit_tile
        count = rows // row_tile * across // parts
        first = rows if phase == 3 else 0
        source = terms_ref(phase)
        goal = hidden_view(size)

        @pl.loop(part * count, (part + 1) * count)
        def _(i):
            start = pl.multiple_of((i // across) * row_tile, row_tile)
            place = pl.ds(start, row_tile)
            cols = columns(i % across, unit_tile)
            gate_value = dot(source[place, :], gate[:, cols])
            up_value = dot(source[place, :], up[:, cols])
            goal[pl.ds(start + first, row_tile), cols] = (
                jax.nn.silu(gate_value) * up_value
            ).astype(BF16)

    def grain(phase):
        return half if phase == 2 and half % 128 == 0 else block

    def pieces(phase):
        return width // grain(phase)

    def near_copy(phase, b):
        q, block = pieces(phase), grain(phase)
        slot = b // q // 2 * q + b % q
        return pltpu.make_async_remote_copy(
            src_ref=terms_ref(phase).at[:, columns(b, block)],
            dst_ref=near_of(phase).at[:, columns(slot, block)],
            send_sem=rs_near_send.at[phase // 3, b],
            recv_sem=rs_near_recv.at[phase, slot],
            device_id={"tp": partner},
            device_id_type=MESH,
        )

    def far_copy(phase, b):
        q, block = pieces(phase), grain(phase)
        to_chip = b // q // 2
        hop = lax.rem(to_chip - chip + chips, chips)
        slot = (hop - 1) * q + b % q
        return pltpu.make_async_remote_copy(
            src_ref=terms_ref(phase).at[:, columns(b, block)],
            dst_ref=far_of(phase).at[:, columns(slot, block)],
            send_sem=rs_far_send.at[phase // 3, b],
            recv_sem=rs_far_recv.at[phase, slot],
            device_id={"tp": to_chip * 2 + core},
            device_id_type=MESH,
        )

    @scoped
    def terms_of(phase, left_ref, weight, b, many=1):
        q, block = pieces(phase), grain(phase)
        first = rows if phase == 3 else 0
        tall = tile_of(rows, 512)
        weights = pl.ds(pl.multiple_of(b * block * many, block), block * many)

        @pl.loop(0, rows // tall)
        def _(i):
            place = pl.ds(pl.multiple_of(i * tall, tall), tall)
            inner = pl.ds(pl.multiple_of(i * tall + first, tall), tall)
            value = dot_last(left_ref[inner, :], weight[weights, :])
            terms_ref(phase)[place, columns(b, block * many)] = value.astype(BF16)

        for e in range(many):

            @pl.when((b * many + e) // q % 2 != core)
            def _():
                near_copy(phase, b * many + e).start()

    @scoped
    def pass_on(phase, b):
        q, block = pieces(phase), grain(phase)
        mine = b // q % 2 == core
        slot = b // q // 2 * q + b % q

        @pl.when(mine)
        def _():
            near_copy(phase, b).wait_recv()

        @pl.when(mine & (b // q // 2 != chip))
        def _():
            @pl.loop(0, rows // row_tile)
            def _(i):
                place = pl.ds(pl.multiple_of(i * row_tile, row_tile), row_tile)
                total = terms_ref(phase)[place, columns(b, block)].astype(F32)
                total = total + near_of(phase)[place, columns(slot, block)].astype(F32)
                terms_ref(phase)[place, columns(b, block)] = total.astype(BF16)

            far_copy(phase, b).start()

    def turn(b):
        return lax.rem(b + (chip + 1) * (n // chips), n)

    def blocks_at(step):
        if step == 0:
            return [fs]
        if step == h:
            return [owner(at + h)]
        return [owner(at - step), owner(at + step)]

    def far_arrived(phase, hop, k):
        q, block = pieces(phase), grain(phase)
        slot = (hop - 1) * q + k
        place = far_of(phase).at[:, slot * block : (slot + 1) * block]
        return pltpu.make_async_remote_copy(
            src_ref=place,
            dst_ref=place,
            send_sem=rs_far_send.at[phase // 3, 0],
            recv_sem=rs_far_recv.at[phase, slot],
            device_id={"tp": partner},
            device_id_type=MESH,
        )

    def sum_of(phase, place):
        total = terms_ref(phase)[place, columns(tp, width)].astype(F32)
        total = total + near_of(phase)[place, columns(chip, width)].astype(F32)
        for hop in range(1, chips):
            total = total + far_of(phase)[place, (hop - 1) * width : hop * width].astype(F32)
        return total

    chunks = 1
    chunk = rows // chunks

    def mate_copy(which, c):
        cols = columns(tp, width)
        part = pl.ds(c * chunk, chunk)
        return pltpu.make_async_remote_copy(
            src_ref=normed_mate.at[part, cols] if which else tokens.at[part],
            dst_ref=from_mate.at[part] if which else gathered_mate.at[part, cols],
            send_sem=mate_send.at[which, c],
            recv_sem=mate_recv.at[which, c],
            device_id={"fs": mate},
            device_id_type=MESH,
        )

    def mate_start(which):
        for c in range(chunks):
            mate_copy(which, c).start()

    def mate_arrived(which):
        for c in range(chunks):
            mate_copy(which, c).wait_recv()

    @scoped
    def finish_mate():
        for hop in range(1, chips):
            for k in range(pieces(3)):
                far_arrived(3, hop, k).wait_recv()

        @pl.loop(0, rows // row_tile)
        def _(i):
            place = pl.ds(pl.multiple_of(i * row_tile, row_tile), row_tile)
            normed_mate[place, columns(tp, width)] = sum_of(3, place).astype(BF16)

        mate_start(1)

    @scoped
    def finish_sum(phase, factor, whole):
        for hop in range(1, chips):
            for k in range(pieces(phase)):
                far_arrived(phase, hop, k).wait_recv()
        if phase == 0 and split:
            mate_arrived(1)
            launch(U2)

        @pl.loop(0, rows // row_tile)
        def _(i):
            place = pl.ds(pl.multiple_of(i * row_tile, row_tile), row_tile)
            total = sum_of(phase, place)
            if phase == 0 and split:
                total = total + from_mate[place, :].astype(F32)
            value = (stream[place, :].astype(F32) + factor * total).astype(BF16)
            stream[place, :] = value
            if whole:
                gathered[place, columns(tp, width)] = value

    @scoped
    def sent_sum(phase):
        q = pieces(phase)
        for b in range(q * m):

            @pl.when(b // q % 2 != core)
            def _():
                near_copy(phase, b).wait_send()

            @pl.when((b // q % 2 == core) & (b // q // 2 != chip))
            def _():
                far_copy(phase, b).wait_send()

    def piece_of(k):
        if k < 6:
            return (*plan[k // 2][:2], k % 2 * half, half)
        return plan[k - 3]

    def part_rows(k, place, beside):
        low, count = piece_of(k)[2:]
        return pl.ds(pl.multiple_of((place * 2 + beside) * block + low, 16), count)

    def own_part(k, place):
        source, _, low, count = piece_of(k)
        if k >= 6:
            return source
        return source.at[low : low + count, columns(share(place), part_units)]

    def spread_copy(k, bits):
        other = flip(line, bits)
        return pltpu.make_async_remote_copy(
            src_ref=own_part(k, other),
            dst_ref=piece_of(k)[1].at[part_rows(k, line, side)],
            send_sem=spread_send.at[k % 3, bits],
            recv_sem=spread_recv.at[k, bits],
            device_id={"fs": other * 2 + side},
            device_id_type=MESH,
        )

    def spread_arrived(k, bits):
        place = piece_of(k)[1].at[part_rows(k, flip(line, bits), side)]
        return pltpu.make_async_remote_copy(
            src_ref=place,
            dst_ref=place,
            send_sem=spread_send.at[k % 3, bits],
            recv_sem=spread_recv.at[k, bits],
            device_id={"fs": mate},
            device_id_type=MESH,
        )

    def cross_copy(k, bits, arriving=False):
        beside = 1 - side if arriving else side
        place = piece_of(k)[1].at[part_rows(k, flip(line, bits), beside)]
        return pltpu.make_async_remote_copy(
            src_ref=own_part(k, line) if bits == 0 and not arriving else place,
            dst_ref=place,
            send_sem=cross_send.at[k, bits],
            recv_sem=cross_recv.at[k, bits],
            device_id={"fs": fs + 1 - 2 * side},
            device_id_type=MESH,
        )

    mixes = range(6, 9)
    last_first = [*range(2, places), 1]

    @scoped
    def cross(k):
        for bits in last_first:
            spread_arrived(k, bits).wait_recv()
            cross_copy(k, bits).start()
            spread_copy(k, bits).wait_send()
            if k + 2 < 6:
                spread_copy(k + 2, bits).start()

    @scoped
    def crossed(*parts):
        for part in parts:
            for bits in range(places):
                cross_copy(part, bits, arriving=True).wait_recv()

    if split:
        for bits in range(1, places):
            spread_copy(0, bits).start()
        for k in range(6):
            cross_copy(k, 0).start()
    else:
        launch(G1, U1)
    gather_start(0, tokens)
    own = [
        pltpu.make_async_copy(tokens, stream, own_sem.at[0]),
        pltpu.make_async_copy(tokens, gathered.at[:, columns(tp, width)], own_sem.at[1]),
    ]
    mine = pl.ds(pl.multiple_of(fs * block, block), block)
    for k in range(9):
        source, buffer, _, _ = plan[k]
        if split and k in (G1, U1, D1):
            source = source.at[:, columns(share(line), part_units)]
        own.append(pltpu.make_async_copy(source, buffer.at[mine], own_sem.at[2 + k]))
    for copy in own:
        copy.start()
    rate_map[...] = jnp.zeros_like(rate_map)
    input_map[...] = jnp.zeros_like(input_map)
    for k in range(lanes // HEAD_DIM):
        part = slice(k * HEAD_DIM, (k + 1) * HEAD_DIM)
        rate_map[part, part] = rate_weight[k]
        input_map[part, part] = input_weight[k]
    lane[0:8, :] = jnp.zeros((8, lanes), F32)
    with jax.named_scope("ownwait"):
        for copy in own:
            copy.wait()

    if split:
        own_cols = gathered_mate.at[:, columns(tp, width)]
        for bits in range(1, places):
            spread_copy(1, bits).start()
        cross(0)
        mate_start(0)
        gather_forward(0)
        cross(1)
        gather_finish(0, tokens)
        normalise(first_gain)
        cross(2)
        with jax.named_scope("matewait"):
            mate_arrived(0)
        gather_start(3, own_cols)
        cross(3)
        cross(4)
        gather_forward(3)
        cross(5)
        for k in mixes:
            for bits in range(1, places):
                spread_copy(k, bits).start()
        gather_finish(3, own_cols)
        normalise(first_gain, 3)
        crossed(0, 1, 2, 3)
        hidden_part(w_gate1, w_up1, 0, 1, 3)
        crossed(4, 5)
        launch(G2)
        for k in mixes:
            cross_copy(k, 0).start()
        for b in range(n):
            terms_of(3, hidden_half, w_down1, turn(b))
            if b:
                pass_on(3, turn(b - 1))
        pass_on(3, turn(n - 1))
        hidden_part(w_gate1, w_up1, 0, 1, 0)

        @pl.when(core == 0)
        def _():
            finish_mate()

        for b in range(n):
            terms_of(0, hidden_half, w_down1, turn(b))
            if b:
                pass_on(0, turn(b - 1))
            if b == n // 2 - 1:
                for k in mixes:
                    cross(k)

                @pl.when(core == 1)
                def _():
                    finish_mate()

        pass_on(0, turn(n - 1))
    else:
        serve(G1, 1)
        gather_forward(0)
        serve(U1, 1)
        gather_finish(0, tokens)
        normalise(first_gain)
        for step in range(2, h + 1):
            serve(G1, step)
            serve(U1, step)
            if step == h - 1:
                launch(D1)
        launch(MI, MB, MO)
        hidden_part(w_gate1, w_up1, 0, 1, 0)
        for b in blocks_at(0):
            terms_of(0, hidden, w_down1, b)
        for step in range(1, h + 1):
            serve(D1, step)
            for b in blocks_at(step):
                terms_of(0, hidden, w_down1, b)
            for k in (MI, MB, MO):
                serve(k, step)
            for b in blocks_at(step - 1):
                pass_on(0, b)
            if step == h - 1:
                launch(G2, U2)
        for b in blocks_at(h):
            pass_on(0, b)
    finish_sum(0, 0.5, True)
    gather_start(1, stream)
    sent_sum(0)
    if split:
        sent_sum(3)

    queue = [(k, step) for step in range(1, h + 1) for k in (G2, U2)]

    def take(count):
        for _ in range(min(count, len(queue))):
            k, step = queue.pop(0)
            serve(k, step)
            if (k, step) == (G2, h):
                launch(D2A)
            if (k, step) == (U2, h):
                launch(D2B)

    take(1)
    gather_forward(1)
    take(1)
    gather_finish(1, stream)
    normalise(mix_gain)
    if split:
        crossed(*mixes)

    @pl.loop(0, rows // row_tile)
    def _(i):
        place = pl.ds(pl.multiple_of(i * row_tile, row_tile), row_tile)
        lower = pl.ds(pl.multiple_of(i * row_tile + 8, 8), row_tile)
        value = dot(normed[place, :], w_in[...])
        lane[lower, :] = value.astype(BF16).astype(F32)
        branch[place, :] = dot(normed[place, :], w_branch[...])

    take(1)
    slope = -rate_scale * jnp.log1p(jnp.exp(-decay_param[...]))
    small = tile_of(rows, 128)
    lane_id = lax.broadcasted_iota(jnp.int32, (small, lanes), 1) // HEAD_DIM

    @pl.loop(0, rows // small)
    def _(i):
        place = pl.ds(pl.multiple_of(i * small, small), small)
        upper = lane[pl.ds(pl.multiple_of(i * small, 8), small + 8), :]
        conv_sum = jnp.zeros((small, lanes), F32)
        for k in range(CONV):
            shifted = pltpu.roll(upper, CONV - 1 - k, 0) if k < CONV - 1 else upper
            conv_sum = conv_sum + shifted[8:, :] * conv_weight[k : k + 1, :].astype(F32)
        conv_out = conv_sum.astype(BF16)
        rate = jax.nn.sigmoid(dot(conv_out, rate_map[...]))
        admit = jax.nn.sigmoid(dot(conv_out, input_map[...]))
        shifts = decay_shift[:, columns(i, small)]
        shifts = jnp.concatenate([shifts] * (8 // shifts.shape[0]), axis=0).T
        shift = jnp.zeros((small, lanes), F32)
        for k in range(lanes // HEAD_DIM):
            shift = jnp.where(lane_id == k, shifts[:, k : k + 1], shift)
        log_decay = rate * slope + shift
        decay[place, :] = jnp.exp(log_decay)
        drive[place, :] = (
            jnp.sqrt(negative_expm1(2.0 * log_decay)) * admit * conv_out.astype(F32)
        )

    lane_tile = tile_of(lanes, 128)
    row_id = lax.broadcasted_iota(jnp.int32, (rows, lane_tile), 0)

    @pl.loop(0, lanes // lane_tile)
    def _(i):
        cols = columns(i, lane_tile)
        factor, state = decay[:, cols], drive[:, cols]
        reach = 1
        while reach < rows:
            inside = row_id >= reach
            state = factor * jnp.where(inside, pltpu.roll(state, reach, 0), 0.0) + state
            if reach * 2 < rows:
                factor = factor * jnp.where(inside, pltpu.roll(factor, reach, 0), 1.0)
            reach *= 2
        mixed[:, cols] = (state * jax.nn.gelu(branch[:, cols])).astype(BF16)

    for b in range(n):
        terms_of(1, mixed, w_out, turn(b))
        if b:
            pass_on(1, turn(b - 1))
    pass_on(1, turn(n - 1))
    take(2)
    finish_sum(1, 1.0, True)
    gather_start(2, stream)
    sent_sum(1)
    take(2 * h)
    gather_forward(2)
    halves = [(k, step) for step in range(1, h + 1) for k in (D2A, D2B)]
    serve(*halves.pop(0))
    gather_finish(2, stream)
    normalise(second_gain)

    parts = tile_of(rows // row_tile, 4, 2)
    for part in range(parts):
        hidden_part(w_gate2, w_up2, part, parts)
        if part != 2:
            serve(*halves.pop(0))
    fine = block // grain(2)
    held = []
    for step in range(h + 1):
        if step <= 2:
            while halves and halves[0][1] <= step:
                serve(*halves.pop(0))
            for b in blocks_at(step):
                terms_of(2, hidden, w_down2, b, fine)
            for b in held:
                pass_on(2, b)
            held = [b * fine + e for b in blocks_at(step) for e in range(fine)]
            continue
        for piece in range(2):
            while halves and (halves[0][1], halves[0][0]) <= (step, D2A + piece):
                serve(*halves.pop(0))
            for b in held:
                pass_on(2, b)
            held = []
            if fine == 1 and piece == 0:
                continue
            fresh = [
                b * fine + e for b in blocks_at(step) for e in ([piece] if fine == 2 else [0])
            ]
            for b in fresh:
                terms_of(2, hidden, w_down2, b)
            for b in fresh:
                pass_on(2, b)
    finish_sum(2, 0.5, False)

    @pl.loop(0, rows // row_tile)
    def _(i):
        place = pl.ds(pl.multiple_of(i * row_tile, row_tile), row_tile)
        values = stream[place, :].astype(F32)
        squares = jnp.sum(values * values, axis=-1, keepdims=True)
        square_own[:, columns(i, row_tile)] = jnp.broadcast_to(squares, (row_tile, 128)).T[:8, :]

    def square_copy(hop):
        return pltpu.make_async_remote_copy(
            src_ref=square_own,
            dst_ref=square_in.at[hop - 1],
            send_sem=sq_send.at[hop],
            recv_sem=sq_recv.at[hop],
            device_id={"tp": lax.rem(tp + hop, m)},
            device_id_type=MESH,
        )

    for hop in range(1, m):
        square_copy(hop).start()
    sent_sum(2)
    for k in range(G2 if split else 0, len(plan)):
        for way in (0, 1):
            for step in range(h):
                ring_copy(k, way, step).wait_send()
    if split:
        for k in range(9):
            for bits in range(places):
                cross_copy(k, bits).wait_send()
        for which in range(2):
            for c in range(chunks):
                mate_copy(which, c).wait_send()
    with jax.named_scope("sqwait"):
        for hop in range(1, m):
            square_copy(hop).wait()

    def out_copy(i):
        place = pl.ds(i * row_tile, row_tile)
        return pltpu.make_async_copy(stream.at[place], out.at[place], own_sem.at[i])

    with jax.named_scope("final"):
        for i in range(rows // row_tile):
            place = slice(i * row_tile, (i + 1) * row_tile)
            squares = square_own[:, place]
            for hop in range(1, m):
                squares = squares + square_in[hop - 1, :, place]
            spread = jnp.broadcast_to(squares[0:1, :], (128, row_tile)).T
            scale = lax.rsqrt(spread[:, 0:1] / d + norm_eps)
            stream[place, :] = (stream[place, :].astype(F32) * scale * final_gain[...]).astype(BF16)
            out_copy(i).start()
    with jax.named_scope("outwait"):
        for i in range(rows // row_tile):
            out_copy(i).wait()


def shards(n, m, *arrays):
    (
        tokens,
        first_gain,
        first_gate,
        first_up,
        first_down,
        mix_gain,
        mix_input,
        mix_branch,
        conv_weight,
        rate_weight,
        input_weight,
        decay_param,
        decay_shift,
        mix_output,
        second_gain,
        second_gate,
        second_up,
        second_down,
        final_gain,
    ) = arrays
    rows, width = tokens.shape
    d = width * m
    units = first_gate.shape[1]
    lanes = mix_input.shape[1]
    h, q, chips = n // 2, n // m, m // 2
    split = units % 256 == 0 and h % 4 == 0 and h & (h - 1) == 0
    part_units = units // 2 if split else units
    hbm = pl.BlockSpec(memory_space=pl.ANY)
    vmem = pl.BlockSpec(memory_space=pltpu.VMEM)
    dma = pltpu.SemaphoreType.DMA
    spare = pltpu.VMEM((16, 128), BF16)
    return pl.pallas_call(
        functools.partial(kernel, n, m, split),
        out_shape=jax.ShapeDtypeStruct((rows, width), BF16),
        in_specs=[hbm] * 10 + [vmem] * 9,
        out_specs=hbm,
        scratch_shapes=[
            pltpu.VMEM((rows, width), BF16),
            *[pltpu.VMEM((d, part_units), BF16)] * 3,
            *[pltpu.VMEM((d, lanes), BF16)] * 3,
            *[pltpu.VMEM((d, units), BF16)] * 3,
            pltpu.VMEM((rows, d), BF16),
            pltpu.VMEM((rows, d), BF16) if split else spare,
            pltpu.VMEM((rows, d), BF16),
            pltpu.VMEM((rows, d), BF16) if split else spare,
            pltpu.VMEM((rows, units), BF16),
            pltpu.VMEM((2 * rows, part_units), BF16) if split else spare,
            pltpu.VMEM((rows, chips * width), BF16),
            pltpu.VMEM((rows, chips * width), BF16) if split else spare,
            pltpu.VMEM((rows, max(chips - 1, 1) * width), BF16),
            pltpu.VMEM((rows, max(chips - 1, 1) * width), BF16) if split else spare,
            pltpu.VMEM((rows, width), BF16) if split else spare,
            pltpu.VMEM((rows, lanes), BF16),
            pltpu.VMEM((rows + 8, lanes), F32),
            pltpu.VMEM((rows, lanes), F32),
            pltpu.VMEM((rows, lanes), F32),
            pltpu.VMEM((rows, lanes), F32),
            pltpu.VMEM((lanes, lanes), BF16),
            pltpu.VMEM((lanes, lanes), BF16),
            pltpu.VMEM((8, rows), F32),
            pltpu.VMEM((m - 1, 8, rows), F32),
            dma((4 if split else 10, 2, h)),
            dma((4 if split else 10, 2, h)),
            dma((11,)),
            dma((4, chips)),
            dma((4, chips)),
            dma((4, chips)),
            dma((4, chips)),
            dma((2, 2 * n)),
            dma((4, n)),
            dma((2, 2 * n)),
            dma((4, max(chips - 1, 1) * q * 2)),
            dma((m,)),
            dma((m,)),
            dma((3, h)),
            dma((9, h)),
            dma((9, h)),
            dma((9, h)),
            dma((2, 1)),
            dma((2, 1)),
        ],
        compiler_params=pltpu.CompilerParams(
            collective_id=0, has_side_effects=True, vmem_limit_bytes=67043328
        ),
        cost_estimate=pl.CostEstimate(
            flops=rows * d * (12 * units + 6 * lanes), bytes_accessed=8 * d * units, transcendentals=0
        ),
    )(
        tokens,
        first_gate,
        first_up,
        first_down,
        mix_input,
        mix_branch,
        mix_output,
        second_gate,
        second_up,
        second_down,
        first_gain[None, :],
        mix_gain[None, :],
        second_gain[None, :],
        conv_weight,
        rate_weight,
        input_weight,
        decay_param[None, :],
        decay_shift.T,
        final_gain[None, :],
    )


def solution(mesh):
    return jax.shard_map(
        functools.partial(shards, mesh.shape["fs"], mesh.shape["tp"]),
        mesh=mesh,
        in_specs=(
            P("fs", "tp"),
            P(),
            P("fs", "tp"),
            P("fs", "tp"),
            P("fs", "tp"),
            P(),
            P("fs", "tp"),
            P("fs", "tp"),
            P(None, "tp"),
            P("tp", None, None),
            P("tp", None, None),
            P("tp"),
            P("fs", "tp"),
            P("fs", "tp"),
            P(),
            P("fs", "tp"),
            P("fs", "tp"),
            P("fs", "tp"),
            P("tp"),
        ),
        out_specs=P("fs", "tp"),
        check_vma=False,
    )
```
